512 devices in a mesh: sp: 16 (over z), dp: 32 (over y, x, core).
Axes of the slice: x: 4, y: 4, z: 16, core: 2. Of those that a mesh axis runs over, the one named last changes fastest.
Arguments:
- inputs: bfloat16 [12288, 2048], P('dp'), may hold values from -6 to 6
- w_value: bfloat16 [2048, 2048], P('dp', 'sp'), may hold values from -0.125 to 0.125
- w_gate: bfloat16 [2048, 2048], P('dp', 'sp'), may hold values from -0.125 to 0.125
- kernel: bfloat16 [31, 2048], P(None, 'sp'), may hold values from -5 to 5
- conv_bias: bfloat16 [2048], P('sp'), may hold values from -1 to 2.5
- ln_gain: bfloat16 [2048], P('sp'), may hold values from 0.099609375 to 1.8984375
- ln_bias: bfloat16 [2048], P('sp'), may hold values from -3 to 3
- w_out: bfloat16 [2048, 2048], P('dp', 'sp'), may hold values from -0.125 to 0.125
- d_out: bfloat16 [12288, 2048], P('dp'), may hold values from -6 to 6
Outputs:
- grad_input: bfloat16 [12288, 2048], P('dp')
- grad_w_value: float32 [2048, 2048], P('dp', 'sp')
- grad_w_gate: float32 [2048, 2048], P('dp', 'sp')
- grad_w_out: float32 [2048, 2048], P('dp', 'sp')
- grad_kernel: float32 [31, 2048], P(None, 'sp')
- grad_conv_bias: float32 [2048], P('sp')
- grad_ln_gain: float32 [2048], P('sp')
- grad_ln_bias: float32 [2048], P('sp')
The draws below stay inside these ranges and needn't reach their ends.
All inputs are finite; a program needn't handle non-finite values.
Results may differ from the reference program's by a relative error of at most 0.017.
Values may be sent and summed in bfloat16 or wider, within the bound.
No kernel may reach another device: no remote copies, remote signals or barrier semaphores. Data moves between devices by JAX's collectives and lax.ppermute only.
A program may use at most 64 MiB of HBM per device.

```python
import jax
import jax.numpy as jnp
from jax import lax

D = 2048
CH = 2048
KW = 31
TOKENS = 12288
CG = 128
N_SP = 16


def draw_kernel(key, part):
    position = jnp.arange(CH, dtype=jnp.float32) / CH
    rough = jax.random.uniform(jax.random.fold_in(key, 11), (CH,), jnp.float32, -0.3, 0.3)
    scale = jnp.exp(jnp.log(5.0) * position + rough)
    base = jnp.clip(jax.random.normal(jax.random.fold_in(key, 12), (KW, CH), jnp.float32), -4.0, 4.0)
    return (base * scale * KW ** (-0.5)).astype(jnp.bfloat16)


def draw_conv_bias(key, part):
    position = jnp.arange(CH, dtype=jnp.float32) / CH
    noise = 0.3 * jnp.clip(jax.random.normal(jax.random.fold_in(key, 21), (CH,), jnp.float32), -3.0, 3.0)
    return (0.2 + position + noise).astype(jnp.bfloat16)


def with_spikes(entries, key, source, target, blocks, factor):
    owner, partner = [(jnp.arange(entries.shape[dim]) // (entries.shape[dim] // blocks)).reshape([-1 if axis == dim else 1 for axis in range(entries.ndim)]) for dim in (source, target)]
    chosen = jax.random.permutation(key, blocks)[partner]
    strong = (owner == chosen) | (owner == (partner + blocks // 2) % blocks)
    return jnp.where(strong, factor * entries, entries)


def steps_of(key, extent, shards, smallest, top_value):
    loudness, own = 1.0, jax.random.fold_in(key, 6)
    for dim, parts in shards:
        heights = jnp.exp(jax.random.uniform(jax.random.fold_in(own, dim), (parts,), jnp.float32, smallest / len(shards), top_value / len(shards)))
        loudness = loudness * jnp.repeat(heights, extent[dim] // parts).reshape([-1 if axis == dim else 1 for axis in range(len(extent))])
    return loudness


def centred(key, shape, width, reach, cuts=(), kind=jnp.bfloat16):
    entries = width * jax.random.normal(key, shape, jnp.float32)
    if cuts:
        entries = entries * steps_of(key, shape, cuts, -0.22, 0.18)
    return jnp.clip(entries, -reach, reach).astype(kind)


def heavy_noise(rng, shape, scale, reach, split, heavy, kind=jnp.bfloat16):
    drawn = scale * jax.random.normal(rng, shape, jnp.float32)
    if split:
        drawn = drawn * steps_of(rng, shape, split, -0.22, 0.18)
    return jnp.clip(with_spikes(drawn, jax.random.fold_in(rng, 3), *heavy), -reach, reach).astype(kind)


def setup_inputs(seed: int = 0) -> dict:
    keys = jax.random.split(jax.random.key(seed), 10)
    inputs = heavy_noise(keys[0], (TOKENS, D), 1.0, 6.0, ((0, 32),), (0, 1, 32, 2.75))
    w_value = centred(keys[1], (D, CH), D ** -0.5, 0.125, ((0, 32), (1, 16)))
    w_gate = centred(keys[2], (D, CH), D ** -0.5, 0.125, ((0, 32), (1, 16)))
    kernel = draw_kernel(jax.random.fold_in(keys[9], 71), 0)
    conv_bias = draw_conv_bias(jax.random.fold_in(keys[9], 71), 0)
    ln_gain = jnp.clip(1.0 + 0.18 * jax.random.normal(keys[5], (CH,), jnp.float32), 0.099609375, 1.8984375).astype(jnp.bfloat16)
    ln_bias = centred(keys[6], (CH,), 0.5, 3.0, ((0, 16),))
    w_out = centred(keys[7], (D, CH), CH ** -0.5, 0.125, ((0, 32), (1, 16)))
    d_out = heavy_noise(keys[8], (TOKENS, D), 1.0, 6.0, ((0, 32),), (0, 1, 32, 2.75))
    return dict(inputs=inputs, w_value=w_value, w_gate=w_gate, kernel=kernel, conv_bias=conv_bias, ln_gain=ln_gain, ln_bias=ln_bias, w_out=w_out, d_out=d_out)


norm_eps = 1e-05

def depthwise(signal, taps):
    out_len = signal.shape[0] - taps.shape[0] + 1
    total = signal[0:out_len] * taps[0]
    for tap_index in range(1, taps.shape[0]):
        total = total + signal[tap_index:tap_index + out_len] * taps[tap_index]
    return total

def silu_slope(pre_act):
    sigma = jax.nn.sigmoid(pre_act)
    return sigma * (1.0 + pre_act * (1.0 - sigma))

def reference(inputs, w_value, w_gate, kernel, conv_bias, ln_gain, ln_bias, w_out, d_out):
    tap_reach = KW - 1
    value_pre = jnp.dot(inputs, w_value, preferred_element_type=jnp.float32)
    gate_pre = jnp.dot(inputs, w_gate, preferred_element_type=jnp.float32)
    gate_sig = jax.nn.sigmoid(gate_pre)
    gated = (value_pre * gate_sig).astype(jnp.bfloat16)
    padded = jnp.pad(gated.astype(jnp.float32), ((tap_reach, 0), (0, 0)))
    taps = kernel.astype(jnp.float32)
    conved = depthwise(padded, taps) + conv_bias.astype(jnp.float32)
    row_mean = lax.optimization_barrier(jnp.mean(conved, axis=1, keepdims=True))
    centered = conved - row_mean
    row_spread = lax.optimization_barrier(jnp.mean(centered * centered, axis=1, keepdims=True))
    inv_scale = lax.rsqrt(row_spread + norm_eps)
    normed = centered * inv_scale
    gain = ln_gain.astype(jnp.float32)
    shifted = normed * gain + ln_bias.astype(jnp.float32)
    activated = (shifted * jax.nn.sigmoid(shifted)).astype(jnp.bfloat16)
    d_activated = jnp.dot(d_out, w_out, preferred_element_type=jnp.float32)
    d_shifted = d_activated * silu_slope(shifted)
    d_normed = d_shifted * gain
    d_conved = inv_scale * (d_normed - lax.optimization_barrier(jnp.mean(d_normed, axis=1, keepdims=True)) - normed * lax.optimization_barrier(jnp.mean(d_normed * normed, axis=1, keepdims=True)))
    grad_ln_gain = lax.optimization_barrier(jnp.sum(d_shifted * normed, axis=0))
    grad_ln_bias = lax.optimization_barrier(jnp.sum(d_shifted, axis=0))
    grad_conv_bias = lax.optimization_barrier(jnp.sum(d_conved, axis=0))
    grad_kernel = jnp.stack([lax.optimization_barrier(jnp.sum(d_conved * padded[tap_index:tap_index + TOKENS], axis=0)) for tap_index in range(KW)])
    padded_back = jnp.pad(d_conved, ((0, tap_reach), (0, 0)))
    d_gated = depthwise(padded_back, taps[::-1])
    d_value = (d_gated * gate_sig).astype(jnp.bfloat16)
    d_gate = (d_gated * value_pre * gate_sig * (1.0 - gate_sig)).astype(jnp.bfloat16)
    value_groups = d_value.reshape(TOKENS, N_SP, CG).transpose(1, 0, 2)
    gate_groups = d_gate.reshape(TOKENS, N_SP, CG).transpose(1, 0, 2)
    wv_groups = w_value.reshape(D, N_SP, CG).transpose(1, 0, 2)
    wg_groups = w_gate.reshape(D, N_SP, CG).transpose(1, 0, 2)
    dims = (((1,), (1,)), ((), ()))

    def add_group(total, pieces):
        part_value, part_gate, weight_value, weight_gate = pieces
        group_part = lax.dot_general(part_value, weight_value, dims, preferred_element_type=jnp.float32) + lax.dot_general(part_gate, weight_gate, dims, preferred_element_type=jnp.float32)
        rounded = lax.optimization_barrier(group_part.astype(jnp.bfloat16))
        return (total + rounded.astype(jnp.float32), None)
    total, unused = lax.scan(add_group, jnp.zeros((TOKENS, D), jnp.float32), (value_groups, gate_groups, wv_groups, wg_groups))
    grad_input = total.astype(jnp.bfloat16)
    grad_w_value = jnp.dot(inputs.T, d_value, preferred_element_type=jnp.float32)
    grad_w_gate = jnp.dot(inputs.T, d_gate, preferred_element_type=jnp.float32)
    grad_w_out = jnp.dot(d_out.T, activated, preferred_element_type=jnp.float32)
    return (grad_input, grad_w_value, grad_w_gate, grad_w_out, grad_kernel, grad_conv_bias, grad_ln_gain, grad_ln_bias)
```

```python
import jax
import jax.numpy as jnp
from jax import lax
from jax.sharding import PartitionSpec as P


norm_eps = 1e-05
bf16 = jnp.bfloat16
f32 = jnp.float32


def shifted(block, axis, distance):
    count = lax.axis_size(axis)
    route = [(i - distance, i) for i in range(count) if 0 <= i - distance < count]
    return lax.ppermute(block, axis, route)


def turned(block, distance):
    count = lax.axis_size("sp")
    return lax.ppermute(block, "sp", [(i, (i + distance) % count) for i in range(count)])


def copies_from_all(shard, axis):
    copies = jnp.broadcast_to(shard, (lax.axis_size(axis), *shard.shape))
    return lax.all_to_all(copies, axis, split_axis=0, concat_axis=0, tiled=True)


def row_total(first, second):
    both = jnp.concatenate([first, second])
    total = jnp.sum(copies_from_all(both, "sp"), axis=0)
    return total[: first.shape[0]], total[first.shape[0] :]


def depthwise(signal, taps):
    out_len = signal.shape[0] - taps.shape[0] + 1
    total = signal[0:out_len] * taps[0]
    for tap_index in range(1, taps.shape[0]):
        total = total + signal[tap_index : tap_index + out_len] * taps[tap_index]
    return total


def row_terms(left_full, right_block):
    return lax.dot_general(
        left_full, right_block, (((0,), (0,)), ((), ())), preferred_element_type=f32
    )


def plus(*terms):
    total = terms[0].astype(f32)
    for term in terms[1:]:
        total = total + term.astype(f32)
    return total.astype(bf16)


def summed_over_sp(cotangent, weights):
    count = lax.axis_size("sp")
    rows = cotangent.shape[0] // count
    me = lax.axis_index("sp")
    blocks = cotangent.reshape(count, rows, -1)
    rolled = lax.dynamic_slice_in_dim(jnp.concatenate([blocks, blocks]), me, count, 0)

    def part(offsets):
        left = jnp.concatenate([rolled[o % count] for o in offsets])
        out = lax.dot_general(
            left, weights, (((1,), (1,)), ((), ())), preferred_element_type=f32
        )
        return out.astype(bf16).reshape(len(offsets), rows, -1)

    up_1 = turned(part([1, 3, 5, 7]), 1)
    down_1 = turned(part([-1, -3, -5, -7]), -1)
    far = turned(part([8]), 2)
    up = part([0, 2, 4, 6])
    down = part([-2, -4, -6])
    up_2 = turned(jnp.stack([plus(up[1], up_1[1]), plus(up[3], up_1[3], far[0])]), 2)
    down_2 = turned(plus(down[0::2], down_1[1::2]), -2)
    up_4 = turned(plus(up[2], up_1[2], up_2[1]), 4)
    down_4 = turned(plus(down[1], down_1[2], down_2[1]), -4)
    return plus(up[0], up_1[0], up_2[0], down_1[0], down_2[0], up_4, down_4)


def gathered_over_sp(own):
    count = lax.axis_size("sp")
    me = lax.axis_index("sp")
    up = own[None]
    down = own[None]
    pieces = [(0, own)]
    up_4, down_4 = turned(up, 4), turned(down, -4)
    up = jnp.concatenate([up, up_4])
    down = jnp.concatenate([down, down_4])
    up_2, down_2 = turned(up, 2), turned(down, -2)
    up = jnp.concatenate([up, up_2])
    down = jnp.concatenate([down, down_2])
    up_1, down_1 = turned(up, 1), turned(down, -1)
    far = turned(up_2[1], 2)
    pieces = [(0, own[None]), (-8, far[None])]
    for offset, k in ((0, 0), (4, 1), (2, 2), (6, 3)):
        if offset:
            pieces.append((-offset, up[k : k + 1]))
            pieces.append((offset, down[k : k + 1]))
        pieces.append((-offset - 1, up_1[k : k + 1]))
        pieces.append((offset + 1, down_1[k : k + 1]))
    out = jnp.zeros((count, *own.shape), own.dtype)
    for offset, piece in pieces:
        out = lax.dynamic_update_slice_in_dim(out, piece, (me + offset + count) % count, 0)
    return out.reshape(count * own.shape[0], own.shape[1])


def body(inputs, w_value, w_gate, kernel, conv_bias, ln_gain, ln_bias, w_out, d_out):
    row_count, features = inputs.shape
    width = w_value.shape[1]
    tap_count = kernel.shape[0]
    tap_reach = tap_count - 1
    channels = width * lax.axis_size("sp")
    dp_count = lax.axis_size("dp")
    shards = jnp.concatenate([w_value, w_gate, w_out], axis=1)
    weights = copies_from_all(shards, "dp").reshape(features, 3 * width)
    w_in = weights[:, : 2 * width]
    pre = jnp.dot(inputs, w_in, preferred_element_type=f32)
    value_pre, gate_pre = pre[:, :width], pre[:, width:]
    d_activated = jnp.dot(d_out, weights[:, 2 * width :], preferred_element_type=f32)
    gate_sig = jax.nn.sigmoid(gate_pre)
    gated = (value_pre * gate_sig).astype(bf16)
    earlier = shifted(gated[row_count - tap_reach :], "dp", 1)
    extended = jnp.concatenate([earlier, gated], axis=0).astype(f32)
    taps = kernel.astype(f32)
    conved = depthwise(extended, taps) + conv_bias.astype(f32)
    first_sum, second_sum = row_total(
        jnp.sum(conved, axis=1), jnp.sum(conved * conved, axis=1)
    )
    row_mean = first_sum / channels
    row_spread = second_sum / channels - row_mean * row_mean
    centered = conved - row_mean[:, None]
    inv_scale = lax.rsqrt(row_spread + norm_eps)[:, None]
    normed = centered * inv_scale
    gain = ln_gain.astype(f32)
    pre_act = normed * gain + ln_bias.astype(f32)
    sig = jax.nn.sigmoid(pre_act)
    activated = (pre_act * sig).astype(bf16)
    d_shifted = d_activated * (sig * (1.0 + pre_act * (1.0 - sig)))
    d_normed = d_shifted * gain
    first_back, second_back = row_total(
        jnp.sum(d_normed, axis=1), jnp.sum(d_normed * normed, axis=1)
    )
    d_conved = inv_scale * (
        d_normed - (first_back / channels)[:, None] - normed * (second_back / channels)[:, None]
    )
    local_gain = jnp.sum(d_shifted * normed, axis=0)
    local_ln_bias = jnp.sum(d_shifted, axis=0)
    local_conv_bias = jnp.sum(d_conved, axis=0)
    local_kernel = jnp.stack(
        [
            jnp.sum(d_conved * extended[k : k + row_count], axis=0)
            for k in range(tap_count)
        ]
    )
    later = shifted(d_conved[:tap_reach], "dp", -1)
    extended_back = jnp.concatenate([d_conved, later], axis=0)
    d_gated = depthwise(extended_back, taps[::-1])
    d_value = (d_gated * gate_sig).astype(bf16)
    d_gate = (d_gated * value_pre * gate_sig * (1.0 - gate_sig)).astype(bf16)
    both = jnp.concatenate([d_value, d_gate], axis=1)
    own_rows = summed_over_sp(both, w_in)
    grad_input = gathered_over_sp(own_rows)

    small = jnp.concatenate(
        [local_kernel, local_conv_bias[None], local_gain[None], local_ln_bias[None]]
    )
    small_rows = -(-small.shape[0] // 8) * 8
    small = jnp.pad(small, ((0, small_rows - small.shape[0]), (0, 0))).astype(bf16)
    per_device = features // dp_count
    tiles = [
        row_terms(inputs, d_value),
        row_terms(inputs, d_gate),
        row_terms(d_out, activated),
    ]
    sent = jnp.concatenate(
        [t.astype(bf16).reshape(dp_count, per_device, width) for t in tiles]
        + [jnp.broadcast_to(small, (dp_count, small_rows, width))],
        axis=1,
    )
    received = lax.all_to_all(sent, "dp", split_axis=0, concat_axis=0, tiled=True)
    total = jnp.sum(received.astype(f32), axis=0)
    grads = [total[k * per_device : (k + 1) * per_device] for k in range(3)]
    rest = total[3 * per_device :]
    return (
        grad_input,
        *grads,
        rest[:tap_count],
        rest[tap_count],
        rest[tap_count + 1],
        rest[tap_count + 2],
    )


def solution(mesh):
    rows, tile, lane = P("dp", None), P("dp", "sp"), P("sp")
    in_specs = (rows, tile, tile, P(None, "sp"), lane, lane, lane, tile, rows)
    out_specs = (rows, tile, tile, tile, P(None, "sp"), lane, lane, lane)
    return jax.shard_map(body, mesh=mesh, in_specs=in_specs, out_specs=out_specs, check_vma=False)
```

```python
import functools

import jax
import jax.numpy as jnp
from jax import lax
from jax.experimental import pallas as pl
from jax.experimental.pallas import tpu as pltpu
from jax.sharding import PartitionSpec as P


norm_eps = 1e-05
bf16 = jnp.bfloat16
f32 = jnp.float32
halo = 32
VMEM = pl.BlockSpec(memory_space=pltpu.VMEM)
ANY = pl.BlockSpec(memory_space=pl.ANY)


def shifted(block, axis, distance):
    count = lax.axis_size(axis)
    route = [(i - distance, i) for i in range(count) if 0 <= i - distance < count]
    return lax.ppermute(block, axis, route)


def turned(block, distance):
    count = lax.axis_size("sp")
    return lax.ppermute(block, "sp", [(i, (i + distance) % count) for i in range(count)])


def copies_from_all(shard, axis):
    copies = jnp.broadcast_to(shard, (lax.axis_size(axis), *shard.shape))
    return lax.all_to_all(copies, axis, split_axis=0, concat_axis=0, tiled=True)


def row_total(stats):
    rows = stats.shape[1]
    total = jnp.sum(copies_from_all(stats[:2].reshape(1, 2 * rows), "sp"), axis=0)
    return total.reshape(2, rows)


def row_terms(left_full, right_block):
    return lax.dot_general(
        left_full, right_block, (((0,), (0,)), ((), ())), preferred_element_type=f32
    )


def plus(*terms):
    total = terms[0].astype(f32)
    for term in terms[1:]:
        total = total + term.astype(f32)
    return total.astype(bf16)


def logistic(x):
    return 1.0 / (1.0 + jnp.exp(-x))


def lane_sums(first, second):
    ones = jnp.ones((8, first.shape[1]), f32)
    dims = (((1,), (1,)), ((), ()))
    a, b = (
        lax.dot_general(
            ones, x, dims, preferred_element_type=f32, precision=lax.Precision.HIGHEST
        )
        for x in (first, second)
    )
    return jnp.where(lax.broadcasted_iota(jnp.int32, a.shape, 0) == 0, a, b)


def columns(first, second):
    shape = (8, first.shape[1])
    row = lax.broadcasted_iota(jnp.int32, shape, 0)
    both = jnp.where(row == 0, jnp.broadcast_to(first, shape), jnp.broadcast_to(second, shape)).T
    return both[:, 0:1], both[:, 1:2]


def all_shifts(ext_ref, sh_ref):
    length = ext_ref.shape[0] - 8
    for r in range(8):
        sh_ref[r, 0:length, :] = ext_ref[r : r + length, :]


def window(sh_ref, offset, start, size):
    base = offset // 8 * 8 + start
    return sh_ref[offset % 8, base : base + size, :]


def convolve(sh_ref, taps_ref, offsets, rows, piece, put):
    for start in range(0, rows, piece):
        total = None
        for k, offset in offsets:
            term = window(sh_ref, offset, start, piece) * taps_ref[k : k + 1, :]
            total = term if total is None else total + term
        put(start, total)


def forward_kernel(taps, gated_ref, earlier_ref, taps_ref, bias_ref, conved_ref, stats_ref, ext_ref, sh_ref):
    rows = gated_ref.shape[0]
    ext_ref[0:halo, :] = earlier_ref[...].astype(f32)
    ext_ref[halo : halo + rows, :] = gated_ref[...].astype(f32)
    ext_ref[halo + rows :, :] = jnp.zeros((8, ext_ref.shape[1]), f32)
    all_shifts(ext_ref, sh_ref)

    def put(start, total):
        conved_ref[start : start + 96, :] = total + bias_ref[...]

    convolve(sh_ref, taps_ref, [(k, halo - taps + 1 + k) for k in range(taps)], rows, 96, put)
    conved = conved_ref[...]
    stats_ref[...] = lane_sums(conved, conved * conved)


def scales(total_ref, channels):
    row_mean = total_ref[0:1, :] / channels
    row_spread = total_ref[1:2, :] / channels - row_mean * row_mean
    return columns(row_mean, lax.rsqrt(row_spread + norm_eps))


def norm_kernel(channels, conved_ref, total_ref, gain_ref, beta_ref, d_act_ref, normed_ref, d_normed_ref, act_ref, stats_ref, small_ref):
    row_mean, inv_scale = scales(total_ref, channels)
    normed = (conved_ref[...] - row_mean) * inv_scale
    gain = gain_ref[...]
    pre_act = normed * gain + beta_ref[...]
    sig = logistic(pre_act)
    act_ref[...] = (pre_act * sig).astype(bf16)
    d_shifted = d_act_ref[...] * (sig * (1.0 + pre_act * (1.0 - sig)))
    d_normed = d_shifted * gain
    normed_ref[...] = normed
    d_normed_ref[...] = d_normed
    stats_ref[...] = lane_sums(d_normed, d_normed * normed)
    shape = small_ref.shape
    row = lax.broadcasted_iota(jnp.int32, shape, 0)
    by_gain = jnp.broadcast_to(jnp.sum(d_shifted * normed, axis=0, keepdims=True), shape)
    by_beta = jnp.broadcast_to(jnp.sum(d_shifted, axis=0, keepdims=True), shape)
    small_ref[...] = jnp.where(row == 0, by_gain, jnp.where(row == 1, by_beta, 0.0))


def conved_kernel(channels, normed_ref, d_normed_ref, total_ref, back_ref, d_conved_ref):
    _, inv_scale = scales(total_ref, channels)
    first, second = columns(back_ref[0:1, :] / channels, back_ref[1:2, :] / channels)
    d_conved_ref[...] = inv_scale * (d_normed_ref[...] - first - normed_ref[...] * second)


def backward_kernel(taps, blocks, d_conved_ref, later_ref, taps_ref, pre_ref, out_ref, ext_ref, sh_ref):
    rows, width = d_conved_ref.shape
    ext_ref[0:rows, :] = d_conved_ref[...]
    ext_ref[rows : rows + halo, :] = later_ref[...]
    ext_ref[rows + halo :, :] = jnp.zeros((8, width), f32)
    all_shifts(ext_ref, sh_ref)
    me = lax.axis_index("sp")
    piece = rows // blocks

    def put(start, d_gated):
        value = pre_ref[start : start + piece, :width]
        sig = logistic(pre_ref[start : start + piece, width:])
        d_value = d_gated * sig
        d_gate = d_value * value * (1.0 - sig)
        away = lax.rem(start // piece - me + blocks, blocks)
        out_ref[lax.rem(away, 4), away // 4] = jnp.concatenate([d_value, d_gate], axis=1).astype(bf16)

    convolve(sh_ref, taps_ref, [(k, taps - 1 - k) for k in range(taps)], rows, piece, put)


def taps_kernel(taps, d_conved_ref, gated_ref, earlier_ref, small_ref, out_ref, ext_ref, sh_ref):
    rows, width = d_conved_ref.shape
    ext_ref[0:halo, :] = earlier_ref[...].astype(f32)
    ext_ref[halo : halo + rows, :] = gated_ref[...].astype(f32)
    ext_ref[halo + rows :, :] = jnp.zeros((8, width), f32)
    all_shifts(ext_ref, sh_ref)

    def folded(x):
        return jnp.sum(x.reshape(rows // 8, 8, width), axis=0)

    d_conved = d_conved_ref[...]
    sums = [
        folded(d_conved * window(sh_ref, halo - taps + 1 + k, 0, rows)) for k in range(taps)
    ]
    sums.append(folded(d_conved))
    sums = [jnp.sum(s, axis=0, keepdims=True) for s in sums]
    out_ref[...] = jnp.concatenate(sums + [small_ref[...]], axis=0).astype(bf16)


def place_kernel(offsets, *refs):
    *pieces, out_ref, sem = refs
    count = out_ref.shape[0]
    me = lax.axis_index("sp")
    copies = []
    at = 0
    for piece, places in zip(pieces, offsets):
        for k, offset in enumerate(places):
            to = lax.rem(me + (offset + count) % count, count)
            copies.append(pltpu.make_async_copy(piece.at[k], out_ref.at[to], sem.at[at]))
            copies[-1].start()
            at += 1
    for copy in copies:
        copy.wait()


def call(kernel, shapes, scratch=(), **how):
    return pl.pallas_call(kernel, out_shape=shapes, scratch_shapes=list(scratch), **how)


def local(kernel, inputs, shapes, scratch=()):
    return pl.pallas_call(
        kernel,
        out_shape=[jax.ShapeDtypeStruct(s, t) for s, t in shapes],
        in_specs=[VMEM] * len(inputs),
        out_specs=[VMEM] * len(shapes),
        scratch_shapes=list(scratch),
    )(*inputs)


def summed_over_sp(blocks, weights):
    rows = blocks.shape[2]

    def part(pieces):
        left = jnp.concatenate([p.reshape(-1, p.shape[-1]) for p in pieces])
        out = lax.dot_general(
            left, weights, (((1,), (1,)), ((), ())), preferred_element_type=f32
        )
        return out.astype(bf16).reshape(-1, rows, out.shape[-1])

    head = part([blocks[3, :2], blocks[1, 2:]])
    up = turned(head[:2], 1)
    down = turned(head[2:], -1)
    rest = part([blocks[0], blocks[2], blocks[1, :2], blocks[3, 2:]])
    far = turned(rest[2:3], 2)
    up = turned(jnp.stack([plus(rest[4], up[0]), plus(rest[5], up[1], far[0])]), 1)
    down = turned(plus(rest[6:8], down), -1)
    up = turned(plus(rest[8:10], up), 1)
    down = turned(plus(rest[10:12], down), -1)
    up_4 = turned(plus(rest[1], up[1]), 4)
    down_4 = turned(plus(rest[3], down[0]), -4)
    return plus(rest[0], up[0], down[1], up_4, down_4)


def gathered_over_sp(own):
    count = lax.axis_size("sp")
    own = own[None]
    up_4, down_4 = turned(own, 4), turned(own, -4)
    up_1 = turned(jnp.concatenate([own, up_4]), 1)
    down_1 = turned(jnp.concatenate([own, down_4]), -1)
    up_2, down_2 = turned(up_1, 1), turned(down_1, -1)
    up_3, down_3 = turned(up_2, 1), turned(down_2, -1)
    far = turned(up_2[1:2], 2)
    pieces = [own, up_4, down_4, up_1, down_1, up_2, down_2, up_3, down_3, far]
    offsets = [(0,), (-4,), (4,), (-1, -5), (1, 5), (-2, -6), (2, 6), (-3, -7), (3, 7), (-8,)]
    out = pl.pallas_call(
        functools.partial(place_kernel, offsets),
        out_shape=jax.ShapeDtypeStruct((count, *own.shape[1:]), own.dtype),
        in_specs=[ANY] * len(pieces),
        out_specs=ANY,
        scratch_shapes=[pltpu.SemaphoreType.DMA((count,))],
    )(*pieces)
    return out.reshape(count * own.shape[1], own.shape[2])


def body(inputs, w_value, w_gate, kernel, conv_bias, ln_gain, ln_bias, w_out, d_out):
    rows, features = inputs.shape
    width = w_value.shape[1]
    taps = kernel.shape[0]
    sp_count, dp_count = lax.axis_size("sp"), lax.axis_size("dp")
    channels = width * sp_count
    shards = jnp.concatenate([w_value, w_gate, w_out], axis=1)
    weights = copies_from_all(shards, "dp").reshape(features, 3 * width)
    w_in = weights[:, : 2 * width]
    pre = jnp.dot(inputs, w_in, preferred_element_type=f32)
    d_activated = jnp.dot(d_out, weights[:, 2 * width :], preferred_element_type=f32)
    gated = (pre[:, :width] * jax.nn.sigmoid(pre[:, width:])).astype(bf16)
    earlier = shifted(gated[rows - halo :], "dp", 1)
    tap_rows = jnp.pad(kernel, ((0, 32 - taps), (0, 0))).astype(f32)
    lane = (1, width)
    bias, gain, beta = (x.astype(f32).reshape(lane) for x in (conv_bias, ln_gain, ln_bias))
    block, stats = ((rows, width), f32), ((8, rows), f32)
    scratch = [
        pltpu.VMEM((rows + halo + 8, width), f32),
        pltpu.VMEM((8, rows + halo, width), f32),
    ]
    conved, sums = local(
        functools.partial(forward_kernel, taps),
        (gated, earlier, tap_rows, bias),
        [block, stats],
        scratch,
    )
    total = row_total(sums)
    normed, d_normed, activated, sums, small = local(
        functools.partial(norm_kernel, channels),
        (conved, total, gain, beta, d_activated),
        [block, block, ((rows, width), bf16), stats, ((8, width), f32)],
    )
    back = row_total(sums)
    (d_conved,) = local(
        functools.partial(conved_kernel, channels), (normed, d_normed, total, back), [block]
    )
    later = shifted(d_conved[:halo], "dp", -1)
    (blocks,) = local(
        functools.partial(backward_kernel, taps, sp_count),
        (d_conved, later, tap_rows, pre),
        [((4, sp_count // 4, rows // sp_count, 2 * width), bf16)],
        scratch,
    )
    grad_input = gathered_over_sp(summed_over_sp(blocks, w_in))

    (small,) = local(
        functools.partial(taps_kernel, taps),
        (d_conved, gated, earlier, small),
        [((40, width), bf16)],
        scratch,
    )
    me = lax.axis_index("sp")
    natural = jnp.swapaxes(blocks, 0, 1).reshape(sp_count, -1, 2 * width)
    natural = lax.dynamic_slice_in_dim(
        jnp.concatenate([natural, natural]), lax.rem(sp_count - me, sp_count), sp_count, 0
    ).reshape(rows, 2 * width)
    per_device = features // dp_count
    both = row_terms(inputs, natural).astype(bf16)
    tiles = [both[:, :width], both[:, width:], row_terms(d_out, activated).astype(bf16)]
    sent = jnp.concatenate(
        [t.reshape(dp_count, per_device, width) for t in tiles]
        + [jnp.broadcast_to(small, (dp_count, *small.shape))],
        axis=1,
    )
    received = lax.all_to_all(sent, "dp", split_axis=0, concat_axis=0, tiled=True)
    summed = jnp.sum(received.astype(f32), axis=0)
    grads = [summed[k * per_device : (k + 1) * per_device] for k in range(3)]
    rest = summed[3 * per_device :]
    return (
        grad_input,
        *grads,
        rest[:taps],
        rest[taps],
        rest[taps + 1],
        rest[taps + 2],
    )


def solution(mesh):
    rows, tile, lane = P("dp", None), P("dp", "sp"), P("sp")
    in_specs = (rows, tile, tile, P(None, "sp"), lane, lane, lane, tile, rows)
    out_specs = (rows, tile, tile, tile, P(None, "sp"), lane, lane, lane)
    return jax.shard_map(body, mesh=mesh, in_specs=in_specs, out_specs=out_specs, check_vma=False)
```

```python
import functools

import jax
import jax.numpy as jnp
from jax import lax
from jax.experimental import pallas as pl
from jax.experimental.pallas import tpu as pltpu
from jax.sharding import PartitionSpec as P


norm_eps = 1e-05
bf16 = jnp.bfloat16
f32 = jnp.float32
halo = 32
VMEM = pl.BlockSpec(memory_space=pltpu.VMEM)
ANY = pl.BlockSpec(memory_space=pl.ANY)


def shifted(block, axis, distance):
    count = lax.axis_size(axis)
    route = [(i - distance, i) for i in range(count) if 0 <= i - distance < count]
    return lax.ppermute(block, axis, route)


def side():
    return 1 - 2 * lax.rem(lax.axis_index("dp"), 2)


def turned(block, distance):
    sp_count, dp_count = lax.axis_size("sp"), lax.axis_size("dp")
    route = [
        (i * dp_count + j, (i + (1 - 2 * (j % 2)) * distance) % sp_count * dp_count + j)
        for i in range(sp_count)
        for j in range(dp_count)
    ]
    return lax.ppermute(block, ("sp", "dp"), route)


def exchanged(copies, axis):
    return lax.all_to_all(copies, axis, split_axis=0, concat_axis=0, tiled=True)


def row_terms(left_full, right_block):
    return lax.dot_general(
        left_full, right_block, (((0,), (0,)), ((), ())), preferred_element_type=f32
    )


def plus(*terms):
    total = terms[0].astype(f32)
    for term in terms[1:]:
        total = total + term.astype(f32)
    return total.astype(bf16)


def logistic(x):
    return 1.0 / (1.0 + jnp.exp(-x))


def put_lane_sums(out_ref, first, second):
    ones = jnp.ones((8, first.shape[1]), f32)
    dims = (((1,), (1,)), ((), ()))
    rows = first.shape[0]
    for at, x in ((0, first), (rows, second)):
        sums = lax.dot_general(
            ones, x, dims, preferred_element_type=f32, precision=lax.Precision.HIGHEST
        )[0:1]
        for k in range(out_ref.shape[0]):
            out_ref[k, :, at : at + rows] = sums


def both_totals(parts_ref):
    total = jnp.sum(parts_ref[...], axis=0)
    rows = total.shape[1] // 2
    return total[:, :rows], total[:, rows:]


def columns(first, second):
    shape = (8, first.shape[1])
    row = lax.broadcasted_iota(jnp.int32, shape, 0)
    both = jnp.where(row == 0, jnp.broadcast_to(first, shape), jnp.broadcast_to(second, shape)).T
    return both[:, 0:1], both[:, 1:2]


def all_shifts(ext_ref, sh_ref):
    length = ext_ref.shape[0] - 8
    for r in range(8):
        sh_ref[r, 0:length, :] = ext_ref[r : r + length, :]


def window(sh_ref, offset, start, size):
    base = offset // 8 * 8 + start
    return sh_ref[offset % 8, base : base + size, :]


def convolve(sh_ref, taps_ref, offsets, rows, piece, put):
    for start in range(0, rows, piece):
        total = None
        for k, offset in offsets:
            term = window(sh_ref, offset, start, piece) * taps_ref[k : k + 1, :]
            total = term if total is None else total + term
        put(start, total)


def forward_kernel(taps, gated_ref, earlier_ref, taps_ref, bias_ref, conved_ref, stats_ref, ext_ref, sh_ref):
    rows = gated_ref.shape[0]
    ext_ref[0:halo, :] = earlier_ref[...].astype(f32)
    ext_ref[halo : halo + rows, :] = gated_ref[...].astype(f32)
    ext_ref[halo + rows :, :] = jnp.zeros((8, ext_ref.shape[1]), f32)
    all_shifts(ext_ref, sh_ref)

    def put(start, total):
        conved_ref[start : start + 96, :] = total + bias_ref[...]

    convolve(sh_ref, taps_ref, [(k, halo - taps + 1 + k) for k in range(taps)], rows, 96, put)
    conved = conved_ref[...]
    put_lane_sums(stats_ref, conved, conved * conved)


def scales(total_ref, channels):
    first, second = both_totals(total_ref)
    row_mean = first / channels
    row_spread = second / channels - row_mean * row_mean
    return columns(row_mean, lax.rsqrt(row_spread + norm_eps))


def norm_kernel(channels, conved_ref, total_ref, gain_ref, beta_ref, d_act_ref, normed_ref, d_normed_ref, act_ref, stats_ref, small_ref):
    row_mean, inv_scale = scales(total_ref, channels)
    normed = (conved_ref[...] - row_mean) * inv_scale
    gain = gain_ref[...]
    pre_act = normed * gain + beta_ref[...]
    sig = logistic(pre_act)
    act_ref[...] = (pre_act * sig).astype(bf16)
    d_shifted = d_act_ref[...] * (sig * (1.0 + pre_act * (1.0 - sig)))
    d_normed = d_shifted * gain
    normed_ref[...] = normed
    d_normed_ref[...] = d_normed
    put_lane_sums(stats_ref, d_normed, d_normed * normed)
    shape = small_ref.shape
    row = lax.broadcasted_iota(jnp.int32, shape, 0)
    by_gain = jnp.broadcast_to(jnp.sum(d_shifted * normed, axis=0, keepdims=True), shape)
    by_beta = jnp.broadcast_to(jnp.sum(d_shifted, axis=0, keepdims=True), shape)
    small_ref[...] = jnp.where(row == 0, by_gain, jnp.where(row == 1, by_beta, 0.0))


def conved_kernel(channels, normed_ref, d_normed_ref, total_ref, back_ref, d_conved_ref):
    _, inv_scale = scales(total_ref, channels)
    first, second = both_totals(back_ref)
    first, second = columns(first / channels, second / channels)
    d_conved_ref[...] = inv_scale * (d_normed_ref[...] - first - normed_ref[...] * second)


def backward_kernel(taps, blocks, d_conved_ref, later_ref, taps_ref, pre_ref, out_ref, natural_ref, ext_ref, sh_ref):
    rows, width = d_conved_ref.shape
    ext_ref[0:rows, :] = d_conved_ref[...]
    ext_ref[rows : rows + halo, :] = later_ref[...]
    ext_ref[rows + halo :, :] = jnp.zeros((8, width), f32)
    all_shifts(ext_ref, sh_ref)
    me, way = lax.axis_index("sp"), side()
    piece = rows // blocks

    def put(start, d_gated):
        value = pre_ref[start : start + piece, :width]
        sig = logistic(pre_ref[start : start + piece, width:])
        d_value = d_gated * sig
        d_gate = d_value * value * (1.0 - sig)
        both = jnp.concatenate([d_value, d_gate], axis=1).astype(bf16)
        away = lax.rem(way * (start // piece - me) + blocks, blocks)
        out_ref[lax.rem(away, 4), away // 4] = both
        natural_ref[start : start + piece, :] = both

    convolve(sh_ref, taps_ref, [(k, taps - 1 - k) for k in range(taps)], rows, piece, put)


def taps_kernel(taps, d_conved_ref, gated_ref, earlier_ref, small_ref, out_ref, ext_ref, sh_ref):
    rows, width = d_conved_ref.shape
    ext_ref[0:halo, :] = earlier_ref[...].astype(f32)
    ext_ref[halo : halo + rows, :] = gated_ref[...].astype(f32)
    ext_ref[halo + rows :, :] = jnp.zeros((8, width), f32)
    all_shifts(ext_ref, sh_ref)

    def folded(x):
        return jnp.sum(x.reshape(rows // 8, 8, width), axis=0)

    d_conved = d_conved_ref[...]
    sums = [
        folded(d_conved * window(sh_ref, halo - taps + 1 + k, 0, rows)) for k in range(taps)
    ]
    sums.append(folded(d_conved))
    sums = [jnp.sum(s, axis=0, keepdims=True) for s in sums]
    out_ref[...] = jnp.concatenate(sums + [small_ref[...]], axis=0).astype(bf16)


def place_kernel(offsets, *refs):
    *pieces, out_ref, sem = refs
    count = out_ref.shape[0]
    me, way = lax.axis_index("sp"), side()
    copies = []
    at = 0
    for piece, places in zip(pieces, offsets):
        for k, offset in enumerate(places):
            to = lax.rem(me + way * offset + count, count)
            copies.append(pltpu.make_async_copy(piece.at[k], out_ref.at[to], sem.at[at]))
            copies[-1].start()
            at += 1
    for copy in copies:
        copy.wait()


def copies_kernel(*refs):
    *shards, out_ref, whole_ref, sem = refs
    at = 0
    for shard in shards:
        whole_ref[:, at : at + shard.shape[1]] = shard[...]
        at += shard.shape[1]
    copies = [
        pltpu.make_async_copy(whole_ref, out_ref.at[k], sem.at[k]) for k in range(out_ref.shape[0])
    ]
    for copy in copies:
        copy.start()
    for copy in copies:
        copy.wait()


def copies_for_all(shards, axis):
    count = lax.axis_size(axis)
    shape = (shards[0].shape[0], sum(s.shape[1] for s in shards))
    return pl.pallas_call(
        copies_kernel,
        out_shape=jax.ShapeDtypeStruct((count, *shape), shards[0].dtype),
        in_specs=[VMEM] * len(shards),
        out_specs=ANY,
        scratch_shapes=[pltpu.VMEM(shape, shards[0].dtype), pltpu.SemaphoreType.DMA((count,))],
    )(*shards)


def weights_kernel(x_ref, y_ref, d_both_ref, act_ref, small_ref, out_ref):
    slots, _, width = out_ref.shape
    each = x_ref.shape[1] // slots
    both = row_terms(x_ref[...], d_both_ref[...]).astype(bf16)
    last = row_terms(y_ref[...], act_ref[...]).astype(bf16)
    for k in range(slots):
        at = slice(k * each, (k + 1) * each)
        out_ref[k, 0:each] = both[at, :width]
        out_ref[k, each : 2 * each] = both[at, width:]
        out_ref[k, 2 * each : 3 * each] = last[at]
        out_ref[k, 3 * each :] = small_ref[...]


def weight_parts(x, y, d_both, act, small, count):
    rows, features = x.shape
    width = act.shape[1]
    each = features // count
    step = min(4, count)
    out = (count, 3 * each + small.shape[0], width)
    wide = pl.BlockSpec((rows, step * each), lambda i: (0, i))

    def full(a):
        return pl.BlockSpec(a.shape, lambda i: (0, 0))

    return pl.pallas_call(
        weights_kernel,
        grid=(count // step,),
        out_shape=jax.ShapeDtypeStruct(out, bf16),
        in_specs=[wide, wide, full(d_both), full(act), full(small)],
        out_specs=pl.BlockSpec((step, *out[1:]), lambda i: (i, 0, 0)),
    )(x, y, d_both, act, small)


def local(kernel, inputs, shapes, scratch=()):
    return pl.pallas_call(
        kernel,
        out_shape=[jax.ShapeDtypeStruct(s, t) for s, t in shapes],
        in_specs=[VMEM] * len(inputs),
        out_specs=[VMEM] * len(shapes),
        scratch_shapes=list(scratch),
    )(*inputs)


def summed_over_sp(blocks, weights):
    rows = blocks.shape[2]

    def part(pieces):
        left = jnp.concatenate([p.reshape(-1, p.shape[-1]) for p in pieces])
        out = lax.dot_general(
            left, weights, (((1,), (1,)), ((), ())), preferred_element_type=f32
        )
        return out.astype(bf16).reshape(-1, rows, out.shape[-1])

    head = part([blocks[3, :2], blocks[1, 2:]])
    up = turned(head[:2], 1)
    down = turned(head[2:], -1)
    rest = part([blocks[0], blocks[2], blocks[1, :2], blocks[3, 2:]])
    far = turned(rest[2:3], 2)
    up = turned(jnp.stack([plus(rest[4], up[0]), plus(rest[5], up[1], far[0])]), 1)
    down = turned(plus(rest[6:8], down), -1)
    up = turned(plus(rest[8:10], up), 1)
    down = turned(plus(rest[10:12], down), -1)
    up_4 = turned(plus(rest[1], up[1]), 4)
    down_4 = turned(plus(rest[3], down[0]), -4)
    return plus(rest[0], up[0], down[1], up_4, down_4), head[0, :8, :128]


def gathered_over_sp(own):
    count = lax.axis_size("sp")
    own = own[None]
    up_4, down_4 = turned(own, 4), turned(own, -4)
    up_1 = turned(jnp.concatenate([own, up_4]), 1)
    down_1 = turned(jnp.concatenate([own, down_4]), -1)
    up_2, down_2 = turned(up_1, 1), turned(down_1, -1)
    up_3, down_3 = turned(up_2, 1), turned(down_2, -1)
    far = turned(up_2[1:2], 2)
    pieces = [own, up_4, down_4, up_1, down_1, up_2, down_2, up_3, down_3, far]
    offsets = [(0,), (-4,), (4,), (-1, -5), (1, 5), (-2, -6), (2, 6), (-3, -7), (3, 7), (-8,)]
    out = pl.pallas_call(
        functools.partial(place_kernel, offsets),
        out_shape=jax.ShapeDtypeStruct((count, *own.shape[1:]), own.dtype),
        in_specs=[VMEM] * len(pieces),
        out_specs=ANY,
        scratch_shapes=[pltpu.SemaphoreType.DMA((count,))],
    )(*pieces)
    return out.reshape(count * own.shape[1], own.shape[2])


def body(inputs, w_value, w_gate, kernel, conv_bias, ln_gain, ln_bias, w_out, d_out):
    rows, features = inputs.shape
    width = w_value.shape[1]
    taps = kernel.shape[0]
    sp_count, dp_count = lax.axis_size("sp"), lax.axis_size("dp")
    channels = width * sp_count
    copies = copies_for_all((w_value, w_gate, w_out), "dp")
    weights = exchanged(copies, "dp").reshape(features, 3 * width)
    w_in = weights[:, : 2 * width]
    pre = jnp.dot(inputs, w_in, preferred_element_type=f32)
    d_activated = jnp.dot(d_out, weights[:, 2 * width :], preferred_element_type=f32)
    gated = (pre[:, :width] * jax.nn.sigmoid(pre[:, width:])).astype(bf16)
    earlier = shifted(gated[rows - halo :], "dp", 1)
    tap_rows = jnp.pad(kernel, ((0, 32 - taps), (0, 0))).astype(f32)
    lane = (1, width)
    bias, gain, beta = (x.astype(f32).reshape(lane) for x in (conv_bias, ln_gain, ln_bias))
    block, stats = ((rows, width), f32), ((sp_count, 1, 2 * rows), f32)
    scratch = [
        pltpu.VMEM((rows + halo + 8, width), f32),
        pltpu.VMEM((8, rows + halo, width), f32),
    ]
    conved, sums = local(
        functools.partial(forward_kernel, taps),
        (gated, earlier, tap_rows, bias),
        [block, stats],
        scratch,
    )
    total = exchanged(sums, "sp")
    normed, d_normed, activated, sums, small = local(
        functools.partial(norm_kernel, channels),
        (conved, total, gain, beta, d_activated),
        [block, block, ((rows, width), bf16), stats, ((8, width), f32)],
    )
    back = exchanged(sums, "sp")
    (d_conved,) = local(
        functools.partial(conved_kernel, channels), (normed, d_normed, total, back), [block]
    )
    later = shifted(d_conved[:halo], "dp", -1)
    blocks, d_both = local(
        functools.partial(backward_kernel, taps, sp_count),
        (d_conved, later, tap_rows, pre),
        [
            ((4, sp_count // 4, rows // sp_count, 2 * width), bf16),
            ((rows, 2 * width), bf16),
        ],
        scratch,
    )
    own_rows, begun = summed_over_sp(blocks, w_in)
    grad_input = gathered_over_sp(own_rows)

    d_conved, _ = lax.optimization_barrier((d_conved, begun))
    (small,) = local(
        functools.partial(taps_kernel, taps),
        (d_conved, gated, earlier, small),
        [((40, width), bf16)],
        scratch,
    )
    per_device = features // dp_count
    sent = weight_parts(inputs, d_out, d_both, activated, small, dp_count)
    received = exchanged(sent, "dp")
    summed = jnp.sum(received.astype(f32), axis=0)
    grads = [summed[k * per_device : (k + 1) * per_device] for k in range(3)]
    rest = summed[3 * per_device :]
    return (
        grad_input,
        *grads,
        rest[:taps],
        rest[taps],
        rest[taps + 1],
        rest[taps + 2],
    )


def solution(mesh):
    rows, tile, lane = P("dp", None), P("dp", "sp"), P("sp")
    in_specs = (rows, tile, tile, P(None, "sp"), lane, lane, lane, tile, rows)
    out_specs = (rows, tile, tile, tile, P(None, "sp"), lane, lane, lane)
    return jax.shard_map(body, mesh=mesh, in_specs=in_specs, out_specs=out_specs, check_vma=False)
```

```python
import functools

import jax
import jax.numpy as jnp
from jax import lax
from jax.experimental import pallas as pl
from jax.experimental.pallas import tpu as pltpu
from jax.sharding import PartitionSpec as P


norm_eps = 1e-05
bf16 = jnp.bfloat16
f32 = jnp.float32
halo = 32
VMEM = pl.BlockSpec(memory_space=pltpu.VMEM)
ANY = pl.BlockSpec(memory_space=pl.ANY)


def shifted(block, axis, distance):
    count = lax.axis_size(axis)
    route = [(i - distance, i) for i in range(count) if 0 <= i - distance < count]
    return lax.ppermute(block, axis, route)


def side():
    return 1 - 2 * lax.rem(lax.axis_index("dp"), 2)


def turned(block, distance):
    sp_count, dp_count = lax.axis_size("sp"), lax.axis_size("dp")
    route = [
        (i * dp_count + j, (i + (1 - 2 * (j % 2)) * distance) % sp_count * dp_count + j)
        for i in range(sp_count)
        for j in range(dp_count)
    ]
    return lax.ppermute(block, ("sp", "dp"), route)


def exchanged(copies, axis):
    return lax.all_to_all(copies, axis, split_axis=0, concat_axis=0, tiled=True)


def row_terms(left_full, right_block):
    return lax.dot_general(
        left_full, right_block, (((0,), (0,)), ((), ())), preferred_element_type=f32
    )


def plus(*terms):
    total = terms[0].astype(f32)
    for term in terms[1:]:
        total = total + term.astype(f32)
    return total.astype(bf16)


def logistic(x):
    return 1.0 / (1.0 + jnp.exp(-x))


def put_lane_sums(out_ref, first, second):
    ones = jnp.ones((8, first.shape[1]), f32)
    dims = (((1,), (1,)), ((), ()))
    rows = first.shape[0]
    out_ref[...] = jnp.zeros(out_ref.shape, f32)
    for at, x in ((0, first), (out_ref.shape[2] // 2, second)):
        sums = lax.dot_general(
            ones, x, dims, preferred_element_type=f32, precision=lax.Precision.HIGHEST
        )[0:1]
        for k in range(out_ref.shape[0]):
            out_ref[k, :, at : at + rows] = sums


def both_totals(parts_ref):
    total = jnp.sum(parts_ref[...], axis=0)
    rows = total.shape[1] // 2
    return total[:, :rows], total[:, rows:]


def columns(first, second, rows):
    shape = (8, first.shape[1])
    row = lax.broadcasted_iota(jnp.int32, shape, 0)
    both = jnp.where(row == 0, jnp.broadcast_to(first, shape), jnp.broadcast_to(second, shape)).T
    return both[:rows, 0:1], both[:rows, 1:2]


def all_shifts(ext_ref, sh_ref):
    length = ext_ref.shape[0] - 8
    for r in range(8):
        sh_ref[r, 0:length, :] = ext_ref[r : r + length, :]


def window(sh_ref, offset, start, size):
    base = offset // 8 * 8 + start
    return sh_ref[offset % 8, base : base + size, :]


def convolve(sh_ref, taps_ref, offsets, rows, piece, put):
    for start in range(0, rows, piece):
        total = None
        for k, offset in offsets:
            term = window(sh_ref, offset, start, piece) * taps_ref[k : k + 1, :]
            total = term if total is None else total + term
        put(start, total)


def forward_kernel(taps, pre_ref, taps_ref, bias_ref, gated_ref, conved_ref, stats_ref, ext_ref, sh_ref):
    length, width = gated_ref.shape
    gated = (pre_ref[:, :width] * logistic(pre_ref[:, width:])).astype(bf16)
    gated_ref[...] = gated
    ext_ref[0:length, :] = gated.astype(f32)
    ext_ref[length:, :] = jnp.zeros((8, width), f32)
    all_shifts(ext_ref, sh_ref)

    def put(start, total):
        conved_ref[start : start + 104, :] = total + bias_ref[...]

    rows = conved_ref.shape[0]
    convolve(sh_ref, taps_ref, [(k, halo - taps + 1 + k) for k in range(taps)], rows, 104, put)
    conved = conved_ref[...]
    put_lane_sums(stats_ref, conved, conved * conved)


def scales(total_ref, channels, rows):
    first, second = both_totals(total_ref)
    row_mean = first / channels
    row_spread = second / channels - row_mean * row_mean
    return columns(row_mean, lax.rsqrt(row_spread + norm_eps), rows)


def norm_kernel(channels, conved_ref, total_ref, gain_ref, beta_ref, d_act_ref, normed_ref, d_normed_ref, act_ref, stats_ref, small_ref):
    own = act_ref.shape[0]
    row_mean, inv_scale = scales(total_ref, channels, conved_ref.shape[0])
    normed = (conved_ref[...] - row_mean) * inv_scale
    gain = gain_ref[...]
    pre_act = normed * gain + beta_ref[...]
    sig = logistic(pre_act)
    act_ref[...] = (pre_act[:own] * sig[:own]).astype(bf16)
    d_shifted = d_act_ref[...] * (sig * (1.0 + pre_act * (1.0 - sig)))
    d_normed = d_shifted * gain
    normed_ref[...] = normed
    d_normed_ref[...] = d_normed
    put_lane_sums(stats_ref, d_normed, d_normed * normed)
    shape = small_ref.shape
    row = lax.broadcasted_iota(jnp.int32, shape, 0)
    by_gain = jnp.sum(d_shifted[:own] * normed[:own], axis=0, keepdims=True)
    by_beta = jnp.sum(d_shifted[:own], axis=0, keepdims=True)
    by_gain, by_beta = jnp.broadcast_to(by_gain, shape), jnp.broadcast_to(by_beta, shape)
    small_ref[...] = jnp.where(row == 0, by_gain, jnp.where(row == 1, by_beta, 0.0))


def place_of(b, a):
    late = jnp.where(b == 0, 4 + a, 8 + a)
    split = jnp.where(a < 2, a, 12 + a)
    return jnp.where(b == 3, split, jnp.where(b == 1, jnp.where(a < 2, 12 + a, a), late))


def backward_kernel(taps, channels, normed_ref, d_normed_ref, total_ref, back_ref, taps_ref, pre_ref, out_ref, natural_ref, d_conved_ref, ext_ref, sh_ref):
    rows, width = d_conved_ref.shape
    blocks = out_ref.shape[0]
    _, inv_scale = scales(total_ref, channels, rows + halo)
    first, second = both_totals(back_ref)
    first, second = columns(first / channels, second / channels, rows + halo)
    d_conved = inv_scale * (d_normed_ref[...] - first - normed_ref[...] * second)
    d_conved_ref[...] = d_conved[:rows]
    ext_ref[0 : rows + halo, :] = d_conved
    ext_ref[rows + halo : rows + halo + 8, :] = jnp.zeros((8, width), f32)
    all_shifts(ext_ref, sh_ref)
    me, way = lax.axis_index("sp"), side()
    piece = rows // blocks

    def put(start, d_gated):
        at = slice(halo + start, halo + start + piece)
        value = pre_ref[at, :width]
        sig = logistic(pre_ref[at, width:])
        d_value = d_gated * sig
        d_gate = d_value * value * (1.0 - sig)
        both = jnp.concatenate([d_value, d_gate], axis=1).astype(bf16)
        away = lax.rem(way * (start // piece - me) + blocks, blocks)
        out_ref[place_of(lax.rem(away, 4), away // 4)] = both
        natural_ref[start : start + piece, :] = both

    convolve(sh_ref, taps_ref, [(k, taps - 1 - k) for k in range(taps)], rows, piece, put)


def taps_kernel(taps, d_conved_ref, gated_ref, small_ref, out_ref, ext_ref, sh_ref):
    rows, width = d_conved_ref.shape
    ext_ref[0 : halo + rows, :] = gated_ref[0 : halo + rows, :].astype(f32)
    ext_ref[halo + rows : halo + rows + 8, :] = jnp.zeros((8, width), f32)
    all_shifts(ext_ref, sh_ref)

    def folded(x):
        return jnp.sum(x.reshape(rows // 8, 8, width), axis=0)

    d_conved = d_conved_ref[...]
    sums = [
        folded(d_conved * window(sh_ref, halo - taps + 1 + k, 0, rows)) for k in range(taps)
    ]
    sums.append(folded(d_conved))
    sums = [jnp.sum(s, axis=0, keepdims=True) for s in sums]
    out_ref[...] = jnp.concatenate(sums + [small_ref[...]], axis=0).astype(bf16)


def power_of_two(exponent):
    size = jnp.abs(exponent).astype(jnp.int32)
    up = down = jnp.ones(exponent.shape, f32)
    for bit in range(7):
        has = lax.rem(lax.shift_right_logical(size, bit), 2) == 1
        up = up * jnp.where(has, f32(2.0 ** 2**bit), f32(1.0))
        down = down * jnp.where(has, f32(2.0 ** -(2**bit)), f32(1.0))
    return jnp.where(exponent < 0, down, up)


def scaled(x, exponent):
    half = jnp.floor(exponent * 0.5)
    return x * power_of_two(half) * power_of_two(exponent - half)


def total_kernel(*refs):
    *parts, out_ref = refs
    features = parts[0].shape[1]
    total = parts[0][...].astype(f32)
    for part in parts[1:]:
        total = total + part[...].astype(f32)
    total = total.astype(bf16).astype(f32)
    top = jnp.max(jnp.max(jnp.abs(total), axis=0, keepdims=True), axis=1, keepdims=True)
    top = jnp.broadcast_to(top, (8, 128))
    exponent = jnp.floor(jnp.log(jnp.maximum(top, 1e-37)) * 1.4426950408889634)
    exponent = 13.0 - jnp.clip(exponent, -126.0, 127.0)
    half = jnp.floor(exponent * 0.5)
    one, two = power_of_two(half)[0:1, 0:1], power_of_two(exponent - half)[0:1, 0:1]
    out_ref[:, :features] = (total * one * two).astype(bf16)
    out_ref[:, features:] = jnp.broadcast_to(exponent[0:1], (out_ref.shape[0], 128)).astype(bf16)


def copies_kernel(*refs):
    *shards, out_ref, whole_ref, sem = refs
    at = 0
    for shard in shards:
        whole_ref[:, at : at + shard.shape[1]] = shard[...]
        at += shard.shape[1]
    copies = [
        pltpu.make_async_copy(whole_ref, out_ref.at[k], sem.at[k]) for k in range(out_ref.shape[0])
    ]
    for copy in copies:
        copy.start()
    for copy in copies:
        copy.wait()


def copies_for_all(shards, axis):
    count = lax.axis_size(axis)
    shape = (shards[0].shape[0], sum(s.shape[1] for s in shards))
    return pl.pallas_call(
        copies_kernel,
        out_shape=jax.ShapeDtypeStruct((count, *shape), shards[0].dtype),
        in_specs=[VMEM] * len(shards),
        out_specs=ANY,
        scratch_shapes=[pltpu.VMEM(shape, shards[0].dtype), pltpu.SemaphoreType.DMA((count,))],
    )(*shards)


def pack_kernel(both_ref, last_ref, small_ref, out_ref):
    slots, _, width = out_ref.shape
    each = both_ref.shape[0] // slots
    for k in range(slots):
        at = slice(k * each, (k + 1) * each)
        out_ref[k, 0:each] = both_ref[at, :width]
        out_ref[k, each : 2 * each] = both_ref[at, width:]
        out_ref[k, 2 * each : 3 * each] = last_ref[at]
        out_ref[k, 3 * each :] = small_ref[...]


def local(kernel, inputs, shapes, scratch=()):
    return pl.pallas_call(
        kernel,
        out_shape=[jax.ShapeDtypeStruct(s, t) for s, t in shapes],
        in_specs=[VMEM] * len(inputs),
        out_specs=[VMEM] * len(shapes),
        scratch_shapes=list(scratch),
    )(*inputs)


def summed_over_sp(blocks, weights):
    rows = blocks.shape[1]

    def part(left):
        out = lax.dot_general(
            left.reshape(-1, left.shape[-1]),
            weights,
            (((1,), (1,)), ((), ())),
            preferred_element_type=f32,
        )
        return out.astype(bf16).reshape(-1, rows, out.shape[-1])

    head = part(blocks[:4])
    up = turned(head[:2], 1)
    down = turned(head[2:], -1)
    rest = part(blocks[4:])
    far = turned(rest[2:3], 2)
    up = turned(jnp.stack([plus(rest[4], up[0]), plus(rest[5], up[1], far[0])]), 1)
    down = turned(plus(rest[6:8], down), -1)
    up = turned(plus(rest[8:10], up), 1)
    down = turned(plus(rest[10:12], down), -1)
    up_4 = turned(plus(rest[1], up[1]), 4)
    down_4 = turned(plus(rest[3], down[0]), -4)
    return (rest[0], up[0], down[1], up_4, down_4), head[0, :8, :128]


def gathered_over_sp(parts):
    rows, features = parts[0].shape
    (own,) = local(total_kernel, parts, [((rows, features + 128), bf16)])
    whole = lax.all_gather(own.astype(jnp.float16), "sp", axis=0, tiled=True).astype(f32)
    exponent = -whole[:, features : features + 1]
    half = jnp.floor(exponent * 0.5)
    one, two = lax.optimization_barrier((power_of_two(half), power_of_two(exponent - half)))
    return (whole[:, :features] * one * two).astype(bf16)


def body(inputs, w_value, w_gate, kernel, conv_bias, ln_gain, ln_bias, w_out, d_out):
    rows, features = inputs.shape
    width = w_value.shape[1]
    taps = kernel.shape[0]
    sp_count, dp_count = lax.axis_size("sp"), lax.axis_size("dp")
    channels = width * sp_count
    copies = copies_for_all((w_value, w_gate, w_out), "dp")
    weights = exchanged(copies, "dp").reshape(features, 3 * width)
    before = shifted(inputs[rows - halo :], "dp", 1)
    after = shifted(inputs[:halo], "dp", -1)
    d_after = shifted(d_out[:halo], "dp", -1)
    inputs_ext = jnp.concatenate([before, inputs, after])
    d_out_ext = jnp.concatenate([d_out, d_after])
    w_in = weights[:, : 2 * width]
    pre = jnp.dot(inputs_ext, w_in, preferred_element_type=f32)
    d_activated = jnp.dot(d_out_ext, weights[:, 2 * width :], preferred_element_type=f32)
    tap_rows = jnp.pad(kernel, ((0, 32 - taps), (0, 0))).astype(f32)
    lane = (1, width)
    bias, gain, beta = (x.astype(f32).reshape(lane) for x in (conv_bias, ln_gain, ln_bias))
    more = rows + halo
    stats_width = -(-more // 128) * 128
    block, stats = ((more, width), f32), ((sp_count, 1, 2 * stats_width), f32)
    scratch = [
        pltpu.VMEM((more + halo + 8, width), f32),
        pltpu.VMEM((8, more + halo, width), f32),
    ]
    gated, conved, sums = local(
        functools.partial(forward_kernel, taps),
        (pre, tap_rows, bias),
        [((more + halo, width), bf16), block, stats],
        scratch,
    )
    total = exchanged(sums, "sp")
    normed, d_normed, activated, sums, small = local(
        functools.partial(norm_kernel, channels),
        (conved, total, gain, beta, d_activated),
        [block, block, ((rows, width), bf16), stats, ((8, width), f32)],
    )
    back = exchanged(sums, "sp")
    blocks, d_both, d_conved = local(
        functools.partial(backward_kernel, taps, channels),
        (normed, d_normed, total, back, tap_rows, pre),
        [
            ((sp_count, rows // sp_count, 2 * width), bf16),
            ((rows, 2 * width), bf16),
            ((rows, width), f32),
        ],
        scratch,
    )
    parts, begun = summed_over_sp(blocks, w_in)
    grad_input = gathered_over_sp(parts)

    d_conved, activated, d_both, _ = lax.optimization_barrier((d_conved, activated, d_both, begun))
    (small,) = local(
        functools.partial(taps_kernel, taps),
        (d_conved, gated, small),
        [((40, width), bf16)],
        scratch,
    )
    per_device = features // dp_count
    (sent,) = local(
        pack_kernel,
        (row_terms(inputs, d_both).astype(bf16), row_terms(d_out, activated).astype(bf16), small),
        [((dp_count, 3 * per_device + small.shape[0], width), bf16)],
    )
    received = exchanged(sent, "dp")
    summed = jnp.sum(received.astype(f32), axis=0)
    grads = [summed[k * per_device : (k + 1) * per_device] for k in range(3)]
    rest = summed[3 * per_device :]
    return (
        grad_input,
        *grads,
        rest[:taps],
        rest[taps],
        rest[taps + 1],
        rest[taps + 2],
    )


def solution(mesh):
    rows, tile, lane = P("dp", None), P("dp", "sp"), P("sp")
    in_specs = (rows, tile, tile, P(None, "sp"), lane, lane, lane, tile, rows)
    out_specs = (rows, tile, tile, tile, P(None, "sp"), lane, lane, lane)
    return jax.shard_map(body, mesh=mesh, in_specs=in_specs, out_specs=out_specs, check_vma=False)
```

```python
import functools

import jax
import jax.numpy as jnp
from jax import lax
from jax.experimental import pallas as pl
from jax.experimental.pallas import tpu as pltpu
from jax.sharding import PartitionSpec as P


norm_eps = 1e-05
bf16 = jnp.bfloat16
f32 = jnp.float32
halo = 32
VMEM = pl.BlockSpec(memory_space=pltpu.VMEM)
ANY = pl.BlockSpec(memory_space=pl.ANY)


def shifted(block, axis, distance):
    count = lax.axis_size(axis)
    route = [(i - distance, i) for i in range(count) if 0 <= i - distance < count]
    return lax.ppermute(block, axis, route)


def side():
    return 1 - 2 * lax.rem(lax.axis_index("dp"), 2)


def turned(block, distance):
    sp_count, dp_count = lax.axis_size("sp"), lax.axis_size("dp")
    route = [
        (i * dp_count + j, (i + (1 - 2 * (j % 2)) * distance) % sp_count * dp_count + j)
        for i in range(sp_count)
        for j in range(dp_count)
    ]
    return lax.ppermute(block, ("sp", "dp"), route)


def exchanged(copies, axis):
    return lax.all_to_all(copies, axis, split_axis=0, concat_axis=0, tiled=True)


def row_terms(left_full, right_block):
    return lax.dot_general(
        left_full, right_block, (((0,), (0,)), ((), ())), preferred_element_type=f32
    )


def plus(*terms):
    total = terms[0].astype(f32)
    for term in terms[1:]:
        total = total + term.astype(f32)
    return total.astype(bf16)


def logistic(x):
    return 1.0 / (1.0 + jnp.exp(-x))


def put_lane_sums(out_ref, first, second):
    ones = jnp.ones((8, first.shape[1]), f32)
    dims = (((1,), (1,)), ((), ()))
    rows = first.shape[0]
    out_ref[...] = jnp.zeros(out_ref.shape, f32)
    for at, x in ((0, first), (out_ref.shape[2] // 2, second)):
        sums = lax.dot_general(
            ones, x, dims, preferred_element_type=f32, precision=lax.Precision.HIGHEST
        )[0:1]
        for k in range(out_ref.shape[0]):
            out_ref[k, :, at : at + rows] = sums


def both_totals(parts_ref):
    total = jnp.sum(parts_ref[...], axis=0)
    rows = total.shape[1] // 2
    return total[:, :rows], total[:, rows:]


def columns(first, second, rows):
    shape = (8, first.shape[1])
    row = lax.broadcasted_iota(jnp.int32, shape, 0)
    both = jnp.where(row == 0, jnp.broadcast_to(first, shape), jnp.broadcast_to(second, shape)).T
    return both[:rows, 0:1], both[:rows, 1:2]


def all_shifts(ext_ref, sh_ref):
    length = ext_ref.shape[0] - 8
    for r in range(8):
        sh_ref[r, 0:length, :] = ext_ref[r : r + length, :]


def window(sh_ref, offset, start, size):
    base = offset // 8 * 8 + start
    return sh_ref[offset % 8, base : base + size, :]


def convolve(sh_ref, taps_ref, offsets, rows, piece, put):
    for start in range(0, rows, piece):
        total = None
        for k, offset in offsets:
            term = window(sh_ref, offset, start, piece) * taps_ref[k : k + 1, :]
            total = term if total is None else total + term
        put(start, total)


def forward_kernel(taps, pre_ref, taps_ref, bias_ref, gated_ref, conved_ref, stats_ref, ext_ref, sh_ref):
    length, width = gated_ref.shape
    gated = (pre_ref[:, :width] * logistic(pre_ref[:, width:])).astype(bf16)
    gated_ref[...] = gated
    ext_ref[0:length, :] = gated.astype(f32)
    ext_ref[length:, :] = jnp.zeros((8, width), f32)
    all_shifts(ext_ref, sh_ref)

    def put(start, total):
        conved_ref[start : start + 104, :] = total + bias_ref[...]

    rows = conved_ref.shape[0]
    convolve(sh_ref, taps_ref, [(k, halo - taps + 1 + k) for k in range(taps)], rows, 104, put)
    conved = conved_ref[...]
    put_lane_sums(stats_ref, conved, conved * conved)


def scales(total_ref, channels, rows):
    first, second = both_totals(total_ref)
    row_mean = first / channels
    row_spread = second / channels - row_mean * row_mean
    return columns(row_mean, lax.rsqrt(row_spread + norm_eps), rows)


def norm_kernel(channels, conved_ref, total_ref, gain_ref, beta_ref, d_act_ref, normed_ref, d_normed_ref, act_ref, stats_ref, small_ref):
    own = act_ref.shape[0]
    row_mean, inv_scale = scales(total_ref, channels, conved_ref.shape[0])
    normed = (conved_ref[...] - row_mean) * inv_scale
    gain = gain_ref[...]
    pre_act = normed * gain + beta_ref[...]
    sig = logistic(pre_act)
    act_ref[...] = (pre_act[:own] * sig[:own]).astype(bf16)
    d_shifted = d_act_ref[...] * (sig * (1.0 + pre_act * (1.0 - sig)))
    d_normed = d_shifted * gain
    normed_ref[...] = normed
    d_normed_ref[...] = d_normed
    put_lane_sums(stats_ref, d_normed, d_normed * normed)
    shape = small_ref.shape
    row = lax.broadcasted_iota(jnp.int32, shape, 0)
    by_gain = jnp.sum(d_shifted[:own] * normed[:own], axis=0, keepdims=True)
    by_beta = jnp.sum(d_shifted[:own], axis=0, keepdims=True)
    by_gain, by_beta = jnp.broadcast_to(by_gain, shape), jnp.broadcast_to(by_beta, shape)
    small_ref[...] = jnp.where(row == 0, by_gain, jnp.where(row == 1, by_beta, 0.0))


def place_of(b, a):
    late = jnp.where(b == 0, 4 + a, 8 + a)
    split = jnp.where(a < 2, a, 12 + a)
    return jnp.where(b == 3, split, jnp.where(b == 1, jnp.where(a < 2, 12 + a, a), late))


def backward_kernel(taps, channels, normed_ref, d_normed_ref, total_ref, back_ref, taps_ref, pre_ref, head_ref, rest_ref, natural_ref, d_conved_ref, ext_ref, sh_ref, out_ref):
    rows, width = d_conved_ref.shape
    blocks = out_ref.shape[0]
    _, inv_scale = scales(total_ref, channels, rows + halo)
    first, second = both_totals(back_ref)
    first, second = columns(first / channels, second / channels, rows + halo)
    d_conved = inv_scale * (d_normed_ref[...] - first - normed_ref[...] * second)
    d_conved_ref[...] = d_conved[:rows]
    ext_ref[0 : rows + halo, :] = d_conved
    ext_ref[rows + halo : rows + halo + 8, :] = jnp.zeros((8, width), f32)
    all_shifts(ext_ref, sh_ref)
    me, way = lax.axis_index("sp"), side()
    piece = rows // blocks

    def put(start, d_gated):
        at = slice(halo + start, halo + start + piece)
        value = pre_ref[at, :width]
        sig = logistic(pre_ref[at, width:])
        d_value = d_gated * sig
        d_gate = d_value * value * (1.0 - sig)
        both = jnp.concatenate([d_value, d_gate], axis=1).astype(bf16)
        away = lax.rem(way * (start // piece - me) + blocks, blocks)
        out_ref[place_of(lax.rem(away, 4), away // 4)] = both
        natural_ref[start : start + piece, :] = both

    convolve(sh_ref, taps_ref, [(k, taps - 1 - k) for k in range(taps)], rows, piece, put)
    heads = head_ref.shape[0] // piece
    for k in range(blocks):
        ref, at = (head_ref, k) if k < heads else (rest_ref, k - heads)
        ref[at * piece : (at + 1) * piece, :] = out_ref[k]


def taps_kernel(taps, d_conved_ref, gated_ref, small_ref, out_ref, ext_ref, sh_ref):
    rows, width = d_conved_ref.shape
    ext_ref[0 : halo + rows, :] = gated_ref[0 : halo + rows, :].astype(f32)
    ext_ref[halo + rows : halo + rows + 8, :] = jnp.zeros((8, width), f32)
    all_shifts(ext_ref, sh_ref)

    def folded(x):
        return jnp.sum(x.reshape(rows // 8, 8, width), axis=0)

    d_conved = d_conved_ref[...]
    sums = [
        folded(d_conved * window(sh_ref, halo - taps + 1 + k, 0, rows)) for k in range(taps)
    ]
    sums.append(folded(d_conved))
    sums = [jnp.sum(s, axis=0, keepdims=True) for s in sums]
    out_ref[...] = jnp.concatenate(sums + [small_ref[...]], axis=0).astype(bf16)


def power_of_two(exponent):
    size = jnp.abs(exponent).astype(jnp.int32)
    up = down = jnp.ones(exponent.shape, f32)
    for bit in range(7):
        has = lax.rem(lax.shift_right_logical(size, bit), 2) == 1
        up = up * jnp.where(has, f32(2.0 ** 2**bit), f32(1.0))
        down = down * jnp.where(has, f32(2.0 ** -(2**bit)), f32(1.0))
    return jnp.where(exponent < 0, down, up)


def scaled(x, exponent):
    half = jnp.floor(exponent * 0.5)
    return x * power_of_two(half) * power_of_two(exponent - half)


def total_kernel(*refs):
    rest_ref, up_ref, down_ref, up_4_ref, down_4_ref, out_ref = refs
    features = rest_ref.shape[2]
    total = rest_ref[0].astype(f32) + up_ref[0].astype(f32) + down_ref[1].astype(f32)
    total = total + up_4_ref[...].astype(f32) + down_4_ref[...].astype(f32)
    total = total.astype(bf16).astype(f32)
    top = jnp.max(jnp.max(jnp.abs(total), axis=0, keepdims=True), axis=1, keepdims=True)
    top = jnp.broadcast_to(top, (8, 128))
    exponent = jnp.floor(jnp.log(jnp.maximum(top, 1e-37)) * 1.4426950408889634)
    exponent = 13.0 - jnp.clip(exponent, -126.0, 127.0)
    half = jnp.floor(exponent * 0.5)
    one, two = power_of_two(half)[0:1, 0:1], power_of_two(exponent - half)[0:1, 0:1]
    out_ref[:, :features] = (total * one * two).astype(bf16)
    out_ref[:, features:] = jnp.broadcast_to(exponent[0:1], (out_ref.shape[0], 128)).astype(bf16)


def copies_kernel(*refs):
    *shards, out_ref, whole_ref, sem = refs
    at = 0
    for shard in shards:
        whole_ref[:, at : at + shard.shape[1]] = shard[...]
        at += shard.shape[1]
    copies = [
        pltpu.make_async_copy(whole_ref, out_ref.at[k], sem.at[k]) for k in range(out_ref.shape[0])
    ]
    for copy in copies:
        copy.start()
    for copy in copies:
        copy.wait()


def merge_kernel(mine_ref, other_ref, first_ref, last_ref):
    core = lax.rem(lax.axis_index("dp"), 2)
    cut = first_ref.shape[3]
    for k in range(first_ref.shape[0]):
        for ref, at in ((mine_ref, core), (other_ref, 1 - core)):
            first_ref[k, at] = ref[k, :, :cut]
            last_ref[k, at] = ref[k, :, cut:]


def gathered_weights(shards):
    count = lax.axis_size("dp")
    copies = copies_for_all(shards, count // 2)
    groups = [list(range(core, count, 2)) for core in range(2)]
    mine = lax.all_to_all(copies, "dp", 0, 0, tiled=True, axis_index_groups=groups)
    other = lax.ppermute(mine, "dp", [(i, i ^ 1) for i in range(count)])
    rows, width = shards[0].shape
    shapes = [((count // 2, 2, rows, n * width), bf16) for n in (2, 1)]
    first, last = local(merge_kernel, (mine, other), shapes)
    return first.reshape(count * rows, -1), last.reshape(count * rows, -1)


def copies_for_all(shards, count):
    shape = (shards[0].shape[0], sum(s.shape[1] for s in shards))
    return pl.pallas_call(
        copies_kernel,
        out_shape=jax.ShapeDtypeStruct((count, *shape), shards[0].dtype),
        in_specs=[VMEM] * len(shards),
        out_specs=ANY,
        scratch_shapes=[pltpu.VMEM(shape, shards[0].dtype), pltpu.SemaphoreType.DMA((count,))],
    )(*shards)


def pack_kernel(both_ref, last_ref, small_ref, out_ref):
    slots, _, width = out_ref.shape
    each = both_ref.shape[0] // slots
    for k in range(slots):
        at = slice(k * each, (k + 1) * each)
        out_ref[k, 0:each] = both_ref[at, :width]
        out_ref[k, each : 2 * each] = both_ref[at, width:]
        out_ref[k, 2 * each : 3 * each] = last_ref[at]
        out_ref[k, 3 * each :] = small_ref[...]


def local(kernel, inputs, shapes, scratch=()):
    return pl.pallas_call(
        kernel,
        out_shape=[jax.ShapeDtypeStruct(s, t) for s, t in shapes],
        in_specs=[VMEM] * len(inputs),
        out_specs=[VMEM] * len(shapes),
        scratch_shapes=list(scratch),
    )(*inputs)


def summed_over_sp(head, rest, rows, weights):
    def part(left):
        out = lax.dot_general(
            left,
            weights,
            (((1,), (1,)), ((), ())),
            preferred_element_type=f32,
        )
        return out.astype(bf16).reshape(-1, rows, out.shape[-1])

    head = part(head)
    up = turned(head[:2], 1)
    down = turned(head[2:], -1)
    rest = part(rest)
    far = turned(rest[2:3], 2)
    up = turned(jnp.stack([plus(rest[4], up[0]), plus(rest[5], up[1], far[0])]), 1)
    down = turned(plus(rest[6:8], down), -1)
    up = turned(plus(rest[8:10], up), 1)
    down = turned(plus(rest[10:12], down), -1)
    up_4 = turned(plus(rest[1], up[1]), 4)
    down_4 = turned(plus(rest[3], down[0]), -4)
    return (rest, up, down, up_4, down_4), head[0, :8, :128]


def undo_kernel(whole_ref, out_ref):
    features = out_ref.shape[1]
    exponent = -whole_ref[:, features:].astype(f32)
    half = jnp.floor(exponent * 0.5)
    one, two = power_of_two(half), power_of_two(exponent - half)
    for at in range(0, features, 128):
        lanes = slice(at, at + 128)
        out_ref[:, lanes] = (whole_ref[:, lanes].astype(f32) * one * two).astype(bf16)


def gathered_over_sp(parts):
    _, rows, features = parts[0].shape
    (own,) = local(total_kernel, parts, [((rows, features + 128), bf16)])
    whole = lax.all_gather(own.astype(jnp.float16), "sp", axis=0, tiled=True).astype(bf16)
    (out,) = local(undo_kernel, (whole,), [((whole.shape[0], features), bf16)])
    return out


def final_kernel(parts_ref, *out_refs):
    total = parts_ref[0].astype(f32)
    for k in range(1, parts_ref.shape[0]):
        total = total + parts_ref[k].astype(f32)
    at = 0
    for ref in out_refs:
        ref[...] = total[at : at + ref.shape[0]]
        at += ref.shape[0]


def body(inputs, w_value, w_gate, kernel, conv_bias, ln_gain, ln_bias, w_out, d_out):
    rows, features = inputs.shape
    width = w_value.shape[1]
    taps = kernel.shape[0]
    sp_count, dp_count = lax.axis_size("sp"), lax.axis_size("dp")
    channels = width * sp_count
    w_in, w_last = gathered_weights((w_value, w_gate, w_out))
    before = shifted(inputs[rows - halo :], "dp", 1)
    after = shifted(inputs[:halo], "dp", -1)
    d_after = shifted(d_out[:halo], "dp", -1)
    inputs_ext = jnp.concatenate([before, inputs, after])
    d_out_ext = jnp.concatenate([d_out, d_after])
    inputs_ext, d_out_ext = lax.optimization_barrier((inputs_ext, d_out_ext))
    pre = jnp.dot(inputs_ext, w_in, preferred_element_type=f32)
    d_activated = jnp.dot(d_out_ext, w_last, preferred_element_type=f32)
    tap_rows = jnp.pad(kernel, ((0, 32 - taps), (0, 0))).astype(f32)
    lane = (1, width)
    bias, gain, beta = (x.astype(f32).reshape(lane) for x in (conv_bias, ln_gain, ln_bias))
    more = rows + halo
    stats_width = -(-more // 128) * 128
    block, stats = ((more, width), f32), ((sp_count, 1, 2 * stats_width), f32)
    scratch = [
        pltpu.VMEM((more + halo + 8, width), f32),
        pltpu.VMEM((8, more + halo, width), f32),
    ]
    gated, conved, sums = local(
        functools.partial(forward_kernel, taps),
        (pre, tap_rows, bias),
        [((more + halo, width), bf16), block, stats],
        scratch,
    )
    total = exchanged(sums, "sp")
    normed, d_normed, activated, sums, small = local(
        functools.partial(norm_kernel, channels),
        (conved, total, gain, beta, d_activated),
        [block, block, ((rows, width), bf16), stats, ((8, width), f32)],
    )
    back = exchanged(sums, "sp")
    piece = rows // sp_count
    head, rest, d_both, d_conved = local(
        functools.partial(backward_kernel, taps, channels),
        (normed, d_normed, total, back, tap_rows, pre),
        [
            ((4 * piece, 2 * width), bf16),
            (((sp_count - 4) * piece, 2 * width), bf16),
            ((rows, 2 * width), bf16),
            ((rows, width), f32),
        ],
        scratch + [pltpu.VMEM((sp_count, piece, 2 * width), bf16)],
    )
    parts, begun = summed_over_sp(head, rest, piece, w_in)
    grad_input = gathered_over_sp(parts)

    d_conved, activated, d_both, _ = lax.optimization_barrier((d_conved, activated, d_both, begun))
    (small,) = local(
        functools.partial(taps_kernel, taps),
        (d_conved, gated, small),
        [((40, width), bf16)],
        scratch,
    )
    per_device = features // dp_count
    (sent,) = local(
        pack_kernel,
        (row_terms(inputs, d_both).astype(bf16), row_terms(d_out, activated).astype(bf16), small),
        [((dp_count, 3 * per_device + small.shape[0], width), bf16)],
    )
    received = exchanged(sent, "dp")
    shapes = [((n, width), f32) for n in [per_device] * 3 + [taps] + [1] * 3]
    *grads, for_bias, for_gain, for_beta = local(final_kernel, (received,), shapes)
    return (grad_input, *grads, *(x.reshape(width) for x in (for_bias, for_gain, for_beta)))


def solution(mesh):
    rows, tile, lane = P("dp", None), P("dp", "sp"), P("sp")
    in_specs = (rows, tile, tile, P(None, "sp"), lane, lane, lane, tile, rows)
    out_specs = (rows, tile, tile, tile, P(None, "sp"), lane, lane, lane)
    return jax.shard_map(body, mesh=mesh, in_specs=in_specs, out_specs=out_specs, check_vma=False)
```

```python
import functools

import jax
import jax.numpy as jnp
from jax import lax
from jax.experimental import pallas as pl
from jax.experimental.pallas import tpu as pltpu
from jax.sharding import PartitionSpec as P


norm_eps = 1e-05
bf16 = jnp.bfloat16
f32 = jnp.float32
halo = 32
VMEM = pl.BlockSpec(memory_space=pltpu.VMEM)
ANY = pl.BlockSpec(memory_space=pl.ANY)


def shifted(block, axis, distance):
    count = lax.axis_size(axis)
    route = [(i - distance, i) for i in range(count) if 0 <= i - distance < count]
    return lax.ppermute(block, axis, route)


def side():
    return 1 - 2 * lax.rem(lax.axis_index("dp"), 2)


def turned(block, distance):
    sp_count, dp_count = lax.axis_size("sp"), lax.axis_size("dp")
    route = [
        (i * dp_count + j, (i + (1 - 2 * (j % 2)) * distance) % sp_count * dp_count + j)
        for i in range(sp_count)
        for j in range(dp_count)
    ]
    return lax.ppermute(block, ("sp", "dp"), route)


def exchanged(copies, axis):
    return lax.all_to_all(copies, axis, split_axis=0, concat_axis=0, tiled=True)


def row_terms(left_full, right_block):
    return lax.dot_general(
        left_full, right_block, (((0,), (0,)), ((), ())), preferred_element_type=f32
    )


def plus(*terms):
    total = terms[0].astype(f32)
    for term in terms[1:]:
        total = total + term.astype(f32)
    return total.astype(bf16)


def logistic(x):
    return 1.0 / (1.0 + jnp.exp(-x))


def put_lane_sums(out_ref, first, second):
    ones = jnp.ones((8, first.shape[1]), f32)
    dims = (((1,), (1,)), ((), ()))
    rows = first.shape[0]
    out_ref[...] = jnp.zeros(out_ref.shape, f32)
    for at, x in ((0, first), (out_ref.shape[2] // 2, second)):
        sums = lax.dot_general(
            ones, x, dims, preferred_element_type=f32, precision=lax.Precision.HIGHEST
        )[0:1]
        for k in range(out_ref.shape[0]):
            out_ref[k, :, at : at + rows] = sums


def both_totals(parts_ref):
    total = jnp.sum(parts_ref[...], axis=0)
    rows = total.shape[1] // 2
    return total[:, :rows], total[:, rows:]


def columns(first, second, rows):
    shape = (8, first.shape[1])
    row = lax.broadcasted_iota(jnp.int32, shape, 0)
    both = jnp.where(row == 0, jnp.broadcast_to(first, shape), jnp.broadcast_to(second, shape)).T
    return both[:rows, 0:1], both[:rows, 1:2]


def all_shifts(ext_ref, sh_ref):
    length = ext_ref.shape[0] - 8
    for r in range(8):
        sh_ref[r, 0:length, :] = ext_ref[r : r + length, :]


def window(sh_ref, offset, start, size):
    base = offset // 8 * 8 + start
    return sh_ref[offset % 8, base : base + size, :]


def convolve(sh_ref, taps_ref, offsets, rows, piece, put):
    for start in range(0, rows, piece):
        total = None
        for k, offset in offsets:
            term = window(sh_ref, offset, start, piece) * taps_ref[k : k + 1, :]
            total = term if total is None else total + term
        put(start, total)


def forward_kernel(taps, x_ref, before_ref, ahead_ref, mine_ref, other_ref, taps_ref, bias_ref, pre_ref, gated_ref, conved_ref, stats_ref, first_ref, last_ref, ext_ref, sh_ref):
    length, width = gated_ref.shape
    rows, features = x_ref.shape
    core = lax.rem(lax.axis_index("dp"), 2)
    for k in range(first_ref.shape[0]):
        for ref, at in ((mine_ref, core), (other_ref, 1 - core)):
            first_ref[k, at] = ref[k, :, : 2 * width]
            last_ref[k, at] = ref[k, :, 2 * width :]
    weights = first_ref[...].reshape(features, 2 * width)
    edges = jnp.concatenate([before_ref[...], ahead_ref[0:halo]])
    edges = jnp.dot(edges, weights, preferred_element_type=f32)
    own = jnp.dot(x_ref[...], weights, preferred_element_type=f32)
    pre_ref[...] = own
    pre = jnp.concatenate([edges[:halo], own, edges[halo:]])
    gated = (pre[:, :width] * logistic(pre[:, width:])).astype(bf16)
    gated_ref[...] = gated
    ext_ref[0:length, :] = gated.astype(f32)
    ext_ref[length:, :] = jnp.zeros((8, width), f32)
    all_shifts(ext_ref, sh_ref)

    def put(start, total):
        conved_ref[start : start + 104, :] = total + bias_ref[...]

    more = conved_ref.shape[0]
    convolve(sh_ref, taps_ref, [(k, halo - taps + 1 + k) for k in range(taps)], more, 104, put)
    conved = conved_ref[...]
    put_lane_sums(stats_ref, conved, conved * conved)


def scales(total_ref, channels, rows):
    first, second = both_totals(total_ref)
    row_mean = first / channels
    row_spread = second / channels - row_mean * row_mean
    return columns(row_mean, lax.rsqrt(row_spread + norm_eps), rows)


def norm_kernel(channels, conved_ref, total_ref, gain_ref, beta_ref, d_act_ref, d_edge_ref, normed_ref, d_normed_ref, act_ref, stats_ref, small_ref):
    own = act_ref.shape[0]
    row_mean, inv_scale = scales(total_ref, channels, conved_ref.shape[0])
    normed = (conved_ref[...] - row_mean) * inv_scale
    gain = gain_ref[...]
    pre_act = normed * gain + beta_ref[...]
    sig = logistic(pre_act)
    act_ref[...] = (pre_act[:own] * sig[:own]).astype(bf16)
    d_act = jnp.concatenate([d_act_ref[...], d_edge_ref[...]])
    d_shifted = d_act * (sig * (1.0 + pre_act * (1.0 - sig)))
    d_normed = d_shifted * gain
    normed_ref[...] = normed
    d_normed_ref[...] = d_normed
    put_lane_sums(stats_ref, d_normed, d_normed * normed)
    shape = small_ref.shape
    row = lax.broadcasted_iota(jnp.int32, shape, 0)
    by_gain = jnp.sum(d_shifted[:own] * normed[:own], axis=0, keepdims=True)
    by_beta = jnp.sum(d_shifted[:own], axis=0, keepdims=True)
    by_gain, by_beta = jnp.broadcast_to(by_gain, shape), jnp.broadcast_to(by_beta, shape)
    small_ref[...] = jnp.where(row == 0, by_gain, jnp.where(row == 1, by_beta, 0.0))


def place_of(b, a):
    late = jnp.where(b == 0, 4 + a, 8 + a)
    split = jnp.where(a < 2, a, 12 + a)
    return jnp.where(b == 3, split, jnp.where(b == 1, jnp.where(a < 2, 12 + a, a), late))


def backward_kernel(taps, channels, normed_ref, d_normed_ref, total_ref, back_ref, taps_ref, pre_ref, up_ref, down_ref, rest_ref, natural_ref, d_conved_ref, ext_ref, sh_ref, out_ref):
    rows, width = d_conved_ref.shape
    blocks = out_ref.shape[0]
    _, inv_scale = scales(total_ref, channels, rows + halo)
    first, second = both_totals(back_ref)
    first, second = columns(first / channels, second / channels, rows + halo)
    d_conved = inv_scale * (d_normed_ref[...] - first - normed_ref[...] * second)
    d_conved_ref[...] = d_conved[:rows]
    ext_ref[0 : rows + halo, :] = d_conved
    ext_ref[rows + halo : rows + halo + 8, :] = jnp.zeros((8, width), f32)
    all_shifts(ext_ref, sh_ref)
    me, way = lax.axis_index("sp"), side()
    piece = rows // blocks

    def put(start, d_gated):
        at = slice(start, start + piece)
        value = pre_ref[at, :width]
        sig = logistic(pre_ref[at, width:])
        d_value = d_gated * sig
        d_gate = d_value * value * (1.0 - sig)
        both = jnp.concatenate([d_value, d_gate], axis=1).astype(bf16)
        away = lax.rem(way * (start // piece - me) + blocks, blocks)
        out_ref[place_of(lax.rem(away, 4), away // 4)] = both
        natural_ref[start : start + piece, :] = both

    convolve(sh_ref, taps_ref, [(k, taps - 1 - k) for k in range(taps)], rows, piece, put)
    for k in range(blocks):
        ref, at = (up_ref, k) if k < 2 else (down_ref, k - 2) if k < 4 else (rest_ref, k - 4)
        ref[at * piece : (at + 1) * piece, :] = out_ref[k]


def taps_kernel(taps, d_conved_ref, gated_ref, small_ref, out_ref, ext_ref, sh_ref):
    rows, width = d_conved_ref.shape
    ext_ref[0 : halo + rows, :] = gated_ref[0 : halo + rows, :].astype(f32)
    ext_ref[halo + rows : halo + rows + 8, :] = jnp.zeros((8, width), f32)
    all_shifts(ext_ref, sh_ref)

    def folded(x):
        return jnp.sum(x.reshape(rows // 8, 8, width), axis=0)

    d_conved = d_conved_ref[...]
    sums = [
        folded(d_conved * window(sh_ref, halo - taps + 1 + k, 0, rows)) for k in range(taps)
    ]
    sums.append(folded(d_conved))
    sums = [jnp.sum(s, axis=0, keepdims=True) for s in sums]
    out_ref[...] = jnp.concatenate(sums + [small_ref[...]], axis=0).astype(bf16)


def power_of_two(exponent):
    size = jnp.abs(exponent).astype(jnp.int32)
    up = down = jnp.ones(exponent.shape, f32)
    for bit in range(7):
        has = jnp.bitwise_and(size, 1 << bit) != 0
        up = up * jnp.where(has, f32(2.0 ** 2**bit), f32(1.0))
        down = down * jnp.where(has, f32(2.0 ** -(2**bit)), f32(1.0))
    return jnp.where(exponent < 0, down, up)


def scaled(x, exponent):
    half = jnp.floor(exponent * 0.5)
    return x * power_of_two(half) * power_of_two(exponent - half)


def total_kernel(*refs):
    rest_ref, up_ref, down_ref, up_4_ref, down_4_ref, out_ref = refs
    features = rest_ref.shape[2]
    total = rest_ref[0].astype(f32) + up_ref[0].astype(f32) + down_ref[1].astype(f32)
    total = total + up_4_ref[...].astype(f32) + down_4_ref[...].astype(f32)
    total = total.astype(bf16).astype(f32)
    top = jnp.max(jnp.max(jnp.abs(total), axis=0, keepdims=True), axis=1, keepdims=True)
    top = jnp.broadcast_to(top, (8, 128))
    exponent = jnp.floor(jnp.log(jnp.maximum(top, 1e-37)) * 1.4426950408889634)
    exponent = 13.0 - jnp.clip(exponent, -126.0, 127.0)
    half = jnp.floor(exponent * 0.5)
    one, two = power_of_two(half)[0:1, 0:1], power_of_two(exponent - half)[0:1, 0:1]
    out_ref[:, :features] = (total * one * two).astype(bf16)
    out_ref[:, features:] = jnp.broadcast_to(exponent[0:1], (out_ref.shape[0], 128)).astype(bf16)


def copies_kernel(*refs):
    *shards, out_ref, whole_ref, sem = refs
    at = 0
    for shard in shards:
        whole_ref[:, at : at + shard.shape[1]] = shard[...]
        at += shard.shape[1]
    copies = [
        pltpu.make_async_copy(whole_ref, out_ref.at[k], sem.at[k]) for k in range(out_ref.shape[0])
    ]
    for copy in copies:
        copy.start()
    for copy in copies:
        copy.wait()


def gathered_weights(shards):
    count = lax.axis_size("dp")
    copies = copies_for_all(shards, count // 2)
    groups = [list(range(core, count, 2)) for core in range(2)]
    mine = lax.all_to_all(copies, "dp", 0, 0, tiled=True, axis_index_groups=groups)
    return mine, lax.ppermute(mine, "dp", [(i, i ^ 1) for i in range(count)])


def copies_for_all(shards, count):
    shape = (shards[0].shape[0], sum(s.shape[1] for s in shards))
    return pl.pallas_call(
        copies_kernel,
        out_shape=jax.ShapeDtypeStruct((count, *shape), shards[0].dtype),
        in_specs=[VMEM] * len(shards),
        out_specs=ANY,
        scratch_shapes=[pltpu.VMEM(shape, shards[0].dtype), pltpu.SemaphoreType.DMA((count,))],
    )(*shards)


def pack_kernel(both_ref, last_ref, small_ref, out_ref):
    slots, _, width = out_ref.shape
    each = both_ref.shape[0] // slots
    for k in range(slots):
        at = slice(k * each, (k + 1) * each)
        out_ref[k, 0:each] = both_ref[at, :width]
        out_ref[k, each : 2 * each] = both_ref[at, width:]
        out_ref[k, 2 * each : 3 * each] = last_ref[at]
        out_ref[k, 3 * each :] = small_ref[...]


def local(kernel, inputs, shapes, scratch=()):
    return pl.pallas_call(
        kernel,
        out_shape=[jax.ShapeDtypeStruct(s, t) for s, t in shapes],
        in_specs=[VMEM] * len(inputs),
        out_specs=[VMEM] * len(shapes),
        scratch_shapes=list(scratch),
    )(*inputs)


def summed_over_sp(up, down, rest, rows, weights):
    def part(left):
        out = lax.dot_general(
            left,
            weights,
            (((1,), (1,)), ((), ())),
            preferred_element_type=f32,
        )
        return out.astype(bf16).reshape(-1, rows, out.shape[-1])

    up, down = part(up), part(down)
    begun = up[0, :8, :128]
    up, down = turned(up, 1), turned(down, -1)
    rest = part(rest)
    far = turned(rest[2:3], 2)
    up = turned(jnp.stack([plus(rest[4], up[0]), plus(rest[5], up[1], far[0])]), 1)
    down = turned(plus(rest[6:8], down), -1)
    up = turned(plus(rest[8:10], up), 1)
    down = turned(plus(rest[10:12], down), -1)
    up_4 = turned(plus(rest[1], up[1]), 4)
    down_4 = turned(plus(rest[3], down[0]), -4)
    return (rest, up, down, up_4, down_4), begun


def undo_kernel(whole_ref, out_ref):
    features = out_ref.shape[1]
    exponent = -whole_ref[:, features:].astype(f32)
    half = jnp.floor(exponent * 0.5)
    one, two = power_of_two(half), power_of_two(exponent - half)
    for at in range(0, features, 128):
        lanes = slice(at, at + 128)
        out_ref[:, lanes] = (whole_ref[:, lanes].astype(f32) * one * two).astype(bf16)


def gathered_over_sp(parts):
    _, rows, features = parts[0].shape
    (own,) = local(total_kernel, parts, [((rows, features + 128), bf16)])
    whole = lax.all_gather(own.astype(jnp.float16), "sp", axis=0, tiled=True).astype(bf16)
    (out,) = local(undo_kernel, (whole,), [((whole.shape[0], features), bf16)])
    return out


def final_kernel(parts_ref, *out_refs):
    total = parts_ref[0].astype(f32)
    for k in range(1, parts_ref.shape[0]):
        total = total + parts_ref[k].astype(f32)
    at = 0
    for ref in out_refs:
        ref[...] = total[at : at + ref.shape[0]]
        at += ref.shape[0]


def body(inputs, w_value, w_gate, kernel, conv_bias, ln_gain, ln_bias, w_out, d_out):
    rows, features = inputs.shape
    width = w_value.shape[1]
    taps = kernel.shape[0]
    sp_count, dp_count = lax.axis_size("sp"), lax.axis_size("dp")
    channels = width * sp_count
    mine, other = gathered_weights((w_value, w_gate, w_out))
    before = shifted(inputs[rows - halo :], "dp", 1)
    ahead = shifted(jnp.concatenate([inputs[:halo], d_out[:halo]]), "dp", -1)
    tap_rows = jnp.pad(kernel, ((0, 32 - taps), (0, 0))).astype(f32)
    lane = (1, width)
    bias, gain, beta = (x.astype(f32).reshape(lane) for x in (conv_bias, ln_gain, ln_bias))
    more = rows + halo
    stats_width = -(-more // 128) * 128
    block, stats = ((more, width), f32), ((sp_count, 1, 2 * stats_width), f32)
    scratch = [
        pltpu.VMEM((more + halo + 8, width), f32),
        pltpu.VMEM((8, more + halo, width), f32),
    ]
    pre, gated, conved, sums, w_in, w_last = local(
        functools.partial(forward_kernel, taps),
        (inputs, before, ahead, mine, other, tap_rows, bias),
        [
            ((rows, 2 * width), f32),
            ((more + halo, width), bf16),
            block,
            stats,
            ((dp_count // 2, 2, features // dp_count, 2 * width), bf16),
            ((dp_count // 2, 2, features // dp_count, width), bf16),
        ],
        scratch,
    )
    w_in, w_last = w_in.reshape(features, 2 * width), w_last.reshape(features, width)
    d_activated = jnp.dot(d_out, w_last, preferred_element_type=f32)
    d_edge = jnp.dot(ahead[halo:], w_last, preferred_element_type=f32)
    total = exchanged(sums, "sp")
    normed, d_normed, activated, sums, small = local(
        functools.partial(norm_kernel, channels),
        (conved, total, gain, beta, d_activated, d_edge),
        [block, block, ((rows, width), bf16), stats, ((8, width), f32)],
    )
    back = exchanged(sums, "sp")
    piece = rows // sp_count
    up, down, rest, d_both, d_conved = local(
        functools.partial(backward_kernel, taps, channels),
        (normed, d_normed, total, back, tap_rows, pre),
        [
            ((2 * piece, 2 * width), bf16),
            ((2 * piece, 2 * width), bf16),
            (((sp_count - 4) * piece, 2 * width), bf16),
            ((rows, 2 * width), bf16),
            ((rows, width), f32),
        ],
        scratch + [pltpu.VMEM((sp_count, piece, 2 * width), bf16)],
    )
    parts, begun = summed_over_sp(up, down, rest, piece, w_in)
    grad_input = gathered_over_sp(parts)

    d_conved, d_both, _ = lax.optimization_barrier((d_conved, d_both, begun))
    (small,) = local(
        functools.partial(taps_kernel, taps),
        (d_conved, gated, small),
        [((40, width), bf16)],
        scratch,
    )
    per_device = features // dp_count
    (sent,) = local(
        pack_kernel,
        (row_terms(inputs, d_both).astype(bf16), row_terms(d_out, activated).astype(bf16), small),
        [((dp_count, 3 * per_device + small.shape[0], width), bf16)],
    )
    received = exchanged(sent, "dp")
    shapes = [((n, width), f32) for n in [per_device] * 3 + [taps] + [1] * 3]
    *grads, for_bias, for_gain, for_beta = local(final_kernel, (received,), shapes)
    return (grad_input, *grads, *(x.reshape(width) for x in (for_bias, for_gain, for_beta)))


def solution(mesh):
    rows, tile, lane = P("dp", None), P("dp", "sp"), P("sp")
    in_specs = (rows, tile, tile, P(None, "sp"), lane, lane, lane, tile, rows)
    out_specs = (rows, tile, tile, tile, P(None, "sp"), lane, lane, lane)
    return jax.shard_map(body, mesh=mesh, in_specs=in_specs, out_specs=out_specs, check_vma=False)
```

```python
import functools

import jax
import jax.numpy as jnp
from jax import lax
from jax.experimental import pallas as pl
from jax.experimental.pallas import tpu as pltpu
from jax.sharding import PartitionSpec as P


norm_eps = 1e-05
bf16 = jnp.bfloat16
f32 = jnp.float32
halo = 32
VMEM = pl.BlockSpec(memory_space=pltpu.VMEM)
ANY = pl.BlockSpec(memory_space=pl.ANY)


def shifted(block, axis, distance):
    count = lax.axis_size(axis)
    route = [(i - distance, i) for i in range(count) if 0 <= i - distance < count]
    return lax.ppermute(block, axis, route)


def side():
    return 1 - 2 * lax.rem(lax.axis_index("dp"), 2)


def turned(block, distance):
    sp_count, dp_count = lax.axis_size("sp"), lax.axis_size("dp")
    route = [
        (i * dp_count + j, (i + (1 - 2 * (j % 2)) * distance) % sp_count * dp_count + j)
        for i in range(sp_count)
        for j in range(dp_count)
    ]
    return lax.ppermute(block, ("sp", "dp"), route)


def exchanged(copies, axis):
    return lax.all_to_all(copies, axis, split_axis=0, concat_axis=0, tiled=True)


def row_terms(left_full, right_block):
    return lax.dot_general(
        left_full, right_block, (((0,), (0,)), ((), ())), preferred_element_type=f32
    )


def plus(*terms):
    total = terms[0].astype(f32)
    for term in terms[1:]:
        total = total + term.astype(f32)
    return total.astype(bf16)


def logistic(x):
    return 1.0 / (1.0 + jnp.exp(-x))


def put_lane_sums(out_ref, first, second):
    ones = jnp.ones((8, first.shape[1]), f32)
    dims = (((1,), (1,)), ((), ()))
    rows = first.shape[0]
    out_ref[...] = jnp.zeros(out_ref.shape, f32)
    for at, x in ((0, first), (out_ref.shape[2] // 2, second)):
        sums = lax.dot_general(
            ones, x, dims, preferred_element_type=f32, precision=lax.Precision.HIGHEST
        )[0:1]
        for k in range(out_ref.shape[0]):
            out_ref[k, :, at : at + rows] = sums


def both_totals(parts_ref):
    total = jnp.sum(parts_ref[...], axis=0)
    rows = total.shape[1] // 2
    return total[:, :rows], total[:, rows:]


def columns(first, second, rows):
    shape = (8, first.shape[1])
    row = lax.broadcasted_iota(jnp.int32, shape, 0)
    both = jnp.where(row == 0, jnp.broadcast_to(first, shape), jnp.broadcast_to(second, shape)).T
    return both[:rows, 0:1], both[:rows, 1:2]


def all_shifts(ext_ref, sh_ref):
    length = ext_ref.shape[0] - 8
    for r in range(8):
        sh_ref[r, 0:length, :] = ext_ref[r : r + length, :]


def window(sh_ref, offset, start, size):
    base = offset // 8 * 8 + start
    return sh_ref[offset % 8, base : base + size, :]


def convolve(sh_ref, taps_ref, offsets, rows, piece, put):
    for start in range(0, rows, piece):
        total = None
        for k, offset in offsets:
            term = window(sh_ref, offset, start, piece) * taps_ref[k : k + 1, :]
            total = term if total is None else total + term
        put(start, total)


def forward_kernel(taps, x_ref, before_ref, ahead_ref, mine_ref, other_ref, taps_ref, bias_ref, pre_ref, gated_ref, conved_ref, stats_ref, first_ref, last_ref, ext_ref, sh_ref):
    length, width = gated_ref.shape
    _, features = x_ref.shape
    core = lax.rem(lax.axis_index("dp"), 2)
    for k in range(first_ref.shape[0]):
        for ref, at in ((mine_ref, core), (other_ref, 1 - core)):
            first_ref[k, at] = ref[k, :, : 2 * width]
            last_ref[k, at] = ref[k, :, 2 * width :]
    weights = first_ref[...].reshape(features, 2 * width)
    edges = jnp.concatenate([before_ref[...], ahead_ref[0:halo]])
    edges = jnp.dot(edges, weights, preferred_element_type=f32)
    own = jnp.dot(x_ref[...], weights, preferred_element_type=f32)
    pre_ref[...] = own
    pre = jnp.concatenate([edges[:halo], own, edges[halo:]])
    gated = (pre[:, :width] * logistic(pre[:, width:])).astype(bf16)
    gated_ref[...] = gated
    ext_ref[0:length, :] = gated.astype(f32)
    ext_ref[length:, :] = jnp.zeros((8, width), f32)
    all_shifts(ext_ref, sh_ref)

    def put(start, total):
        conved_ref[start : start + 104, :] = total + bias_ref[...]

    more = conved_ref.shape[0]
    convolve(sh_ref, taps_ref, [(k, halo - taps + 1 + k) for k in range(taps)], more, 104, put)
    conved = conved_ref[...]
    put_lane_sums(stats_ref, conved, conved * conved)


def scales(total_ref, channels, rows):
    first, second = both_totals(total_ref)
    row_mean = first / channels
    row_spread = second / channels - row_mean * row_mean
    return columns(row_mean, lax.rsqrt(row_spread + norm_eps), rows)


def norm_kernel(channels, conved_ref, total_ref, gain_ref, beta_ref, d_act_ref, d_edge_ref, normed_ref, d_normed_ref, act_ref, stats_ref, small_ref):
    own = act_ref.shape[0]
    row_mean, inv_scale = scales(total_ref, channels, conved_ref.shape[0])
    normed = (conved_ref[...] - row_mean) * inv_scale
    gain = gain_ref[...]
    pre_act = normed * gain + beta_ref[...]
    sig = logistic(pre_act)
    act_ref[...] = (pre_act[:own] * sig[:own]).astype(bf16)
    d_act = jnp.concatenate([d_act_ref[...], d_edge_ref[...]])
    d_shifted = d_act * (sig * (1.0 + pre_act * (1.0 - sig)))
    d_normed = d_shifted * gain
    normed_ref[...] = normed
    d_normed_ref[...] = d_normed
    put_lane_sums(stats_ref, d_normed, d_normed * normed)
    shape = small_ref.shape
    row = lax.broadcasted_iota(jnp.int32, shape, 0)
    by_gain = jnp.sum(d_shifted[:own] * normed[:own], axis=0, keepdims=True)
    by_beta = jnp.sum(d_shifted[:own], axis=0, keepdims=True)
    by_gain, by_beta = jnp.broadcast_to(by_gain, shape), jnp.broadcast_to(by_beta, shape)
    small_ref[...] = jnp.where(row == 0, by_gain, jnp.where(row == 1, by_beta, 0.0))


def place_of(b, a):
    late = jnp.where(b == 0, 4 + a, 8 + a)
    split = jnp.where(a < 2, a, 12 + a)
    return jnp.where(b == 3, split, jnp.where(b == 1, jnp.where(a < 2, 12 + a, a), late))


def backward_kernel(taps, channels, normed_ref, d_normed_ref, total_ref, back_ref, taps_ref, pre_ref, w_in_ref, up_ref, down_ref, rest_ref, natural_ref, d_conved_ref, ext_ref, sh_ref, out_ref):
    rows, width = d_conved_ref.shape
    blocks = out_ref.shape[0]
    _, inv_scale = scales(total_ref, channels, rows + halo)
    first, second = both_totals(back_ref)
    first, second = columns(first / channels, second / channels, rows + halo)
    d_conved = inv_scale * (d_normed_ref[...] - first - normed_ref[...] * second)
    d_conved_ref[...] = d_conved[:rows]
    ext_ref[0 : rows + halo, :] = d_conved
    ext_ref[rows + halo : rows + halo + 8, :] = jnp.zeros((8, width), f32)
    all_shifts(ext_ref, sh_ref)
    me, way = lax.axis_index("sp"), side()
    piece = rows // blocks

    def put(start, d_gated):
        at = slice(start, start + piece)
        value = pre_ref[at, :width]
        sig = logistic(pre_ref[at, width:])
        d_value = d_gated * sig
        d_gate = d_value * value * (1.0 - sig)
        both = jnp.concatenate([d_value, d_gate], axis=1).astype(bf16)
        away = lax.rem(way * (start // piece - me) + blocks, blocks)
        out_ref[place_of(lax.rem(away, 4), away // 4)] = both
        natural_ref[start : start + piece, :] = both

    convolve(sh_ref, taps_ref, [(k, taps - 1 - k) for k in range(taps)], rows, piece, put)
    head = jnp.concatenate([out_ref[k] for k in range(4)])
    head = lax.dot_general(
        head, w_in_ref[...], (((1,), (1,)), ((), ())), preferred_element_type=f32
    ).astype(bf16)
    for k in range(4):
        (up_ref if k < 2 else down_ref)[k % 2] = head[k * piece : (k + 1) * piece]
    for k in range(4, blocks):
        rest_ref[(k - 4) * piece : (k - 3) * piece, :] = out_ref[k]


def taps_kernel(taps, d_conved_ref, gated_ref, small_ref, d_both_ref, after_ref, out_ref, d_same_ref, ext_ref, sh_ref):
    d_same_ref[...] = d_both_ref[...]
    rows, width = d_conved_ref.shape
    ext_ref[0 : halo + rows, :] = gated_ref[0 : halo + rows, :].astype(f32)
    ext_ref[halo + rows : halo + rows + 8, :] = jnp.zeros((8, width), f32)
    all_shifts(ext_ref, sh_ref)

    def folded(x):
        return jnp.sum(x.reshape(rows // 8, 8, width), axis=0)

    d_conved = d_conved_ref[...]
    sums = [
        folded(d_conved * window(sh_ref, halo - taps + 1 + k, 0, rows)) for k in range(taps)
    ]
    sums.append(folded(d_conved))
    sums = [jnp.sum(s, axis=0, keepdims=True) for s in sums]
    out_ref[...] = jnp.concatenate(sums + [small_ref[...]], axis=0).astype(bf16)


def power_of_two(exponent):
    size = jnp.abs(exponent).astype(jnp.int32)
    up = down = jnp.ones(exponent.shape, f32)
    for bit in range(7):
        has = jnp.bitwise_and(size, 1 << bit) != 0
        up = up * jnp.where(has, f32(2.0 ** 2**bit), f32(1.0))
        down = down * jnp.where(has, f32(2.0 ** -(2**bit)), f32(1.0))
    return jnp.where(exponent < 0, down, up)


def total_kernel(*refs):
    *parts, out_ref = refs
    features = parts[0].shape[1]
    total = parts[0][...].astype(f32)
    for part in parts[1:]:
        total = total + part[...].astype(f32)
    total = total.astype(bf16).astype(f32)
    top = jnp.max(jnp.max(jnp.abs(total), axis=0, keepdims=True), axis=1, keepdims=True)
    top = jnp.broadcast_to(top, (8, 128))
    exponent = jnp.floor(jnp.log(jnp.maximum(top, 1e-37)) * 1.4426950408889634)
    exponent = 13.0 - jnp.clip(exponent, -126.0, 127.0)
    half = jnp.floor(exponent * 0.5)
    one, two = power_of_two(half)[0:1, 0:1], power_of_two(exponent - half)[0:1, 0:1]
    out_ref[:, :features] = (total * one * two).astype(bf16)
    out_ref[:, features:] = jnp.broadcast_to(exponent[0:1], (out_ref.shape[0], 128)).astype(bf16)


def copies_kernel(*refs):
    *shards, out_ref, whole_ref, sem = refs
    at = 0
    for shard in shards:
        whole_ref[:, at : at + shard.shape[1]] = shard[...]
        at += shard.shape[1]
    copies = [
        pltpu.make_async_copy(whole_ref, out_ref.at[k], sem.at[k]) for k in range(out_ref.shape[0])
    ]
    for copy in copies:
        copy.start()
    for copy in copies:
        copy.wait()


def from_same_core(shards):
    count = lax.axis_size("dp")
    copies = copies_for_all(shards, count // 2)
    groups = [list(range(core, count, 2)) for core in range(2)]
    return lax.all_to_all(copies, "dp", 0, 0, tiled=True, axis_index_groups=groups)


def copies_for_all(shards, count):
    shape = (shards[0].shape[0], sum(s.shape[1] for s in shards))
    return pl.pallas_call(
        copies_kernel,
        out_shape=jax.ShapeDtypeStruct((count, *shape), shards[0].dtype),
        in_specs=[VMEM] * len(shards),
        out_specs=ANY,
        scratch_shapes=[pltpu.VMEM(shape, shards[0].dtype), pltpu.SemaphoreType.DMA((count,))],
    )(*shards)


def pack_kernel(both_ref, last_ref, small_ref, out_ref):
    slots, _, width = out_ref.shape
    each = both_ref.shape[0] // slots
    for k in range(slots):
        at = slice(k * each, (k + 1) * each)
        out_ref[k, 0:each] = both_ref[at, :width]
        out_ref[k, each : 2 * each] = both_ref[at, width:]
        out_ref[k, 2 * each : 3 * each] = last_ref[at]
        out_ref[k, 3 * each :] = small_ref[...]


def local(kernel, inputs, shapes, scratch=(), in_specs=None):
    return pl.pallas_call(
        kernel,
        out_shape=[jax.ShapeDtypeStruct(s, t) for s, t in shapes],
        in_specs=in_specs or [VMEM] * len(inputs),
        out_specs=[VMEM] * len(shapes),
        scratch_shapes=list(scratch),
    )(*inputs)


def summed_over_sp(up, down, rest, rows, weights):
    def part(left):
        out = lax.dot_general(
            left,
            weights,
            (((1,), (1,)), ((), ())),
            preferred_element_type=f32,
        )
        return out.astype(bf16).reshape(-1, rows, out.shape[-1])

    up, down = turned(up, 1), turned(down, -1)
    rest = part(rest)
    far = turned(rest[2:3], 2)
    up = turned(jnp.stack([plus(rest[4], up[0]), plus(rest[5], up[1], far[0])]), 1)
    down = turned(plus(rest[6:8], down), -1)
    up = turned(plus(rest[8:10], up), 1)
    down = turned(plus(rest[10:12], down), -1)
    begun = down
    up_4 = turned(plus(rest[1], up[1]), 4)
    down_4 = turned(plus(rest[3], down[0]), -4)
    return (rest[0], up[0], down[1], up_4, down_4), begun


def gathered_over_sp(parts):
    rows, features = parts[0].shape
    (own,) = local(total_kernel, parts, [((rows, features + 128), bf16)])
    whole = lax.all_gather(own.astype(jnp.float16), "sp", axis=0, tiled=True)
    blocks = whole.reshape(-1, rows, features + 128)
    exponent = -blocks[:, 0, features].astype(f32)
    half = jnp.floor(exponent * 0.5)
    one, two = lax.optimization_barrier((power_of_two(half), power_of_two(exponent - half)))
    out = blocks[:, :, :features].astype(f32) * one[:, None, None] * two[:, None, None]
    return out.astype(bf16).reshape(-1, features)


def final_kernel(parts_ref, *out_refs):
    total = parts_ref[0].astype(f32)
    for k in range(1, parts_ref.shape[0]):
        total = total + parts_ref[k].astype(f32)
    at = 0
    for ref in out_refs:
        ref[...] = total[at : at + ref.shape[0]]
        at += ref.shape[0]


def body(inputs, w_value, w_gate, kernel, conv_bias, ln_gain, ln_bias, w_out, d_out):
    rows, features = inputs.shape
    width = w_value.shape[1]
    taps = kernel.shape[0]
    sp_count, dp_count = lax.axis_size("sp"), lax.axis_size("dp")
    channels = width * sp_count
    mine = from_same_core((w_value, w_gate, w_out))
    before = shifted(inputs[rows - halo :], "dp", 1)
    ahead = shifted(jnp.concatenate([inputs[:halo], d_out[:halo]]), "dp", -1)
    tap_rows = jnp.pad(kernel, ((0, 32 - taps), (0, 0))).astype(f32)
    lane = (1, width)
    bias, gain, beta = (x.astype(f32).reshape(lane) for x in (conv_bias, ln_gain, ln_bias))
    mine, before, ahead, tap_rows, bias, gain, beta = lax.optimization_barrier(
        (mine, before, ahead, tap_rows, bias, gain, beta)
    )
    other = lax.ppermute(mine, "dp", [(i, i ^ 1) for i in range(dp_count)])
    more = rows + halo
    stats_width = -(-more // 128) * 128
    block, stats = ((more, width), f32), ((sp_count, 1, 2 * stats_width), f32)
    scratch = [
        pltpu.VMEM((more + halo + 8, width), f32),
        pltpu.VMEM((8, more + halo, width), f32),
    ]
    pre, gated, conved, sums, w_in, w_last = local(
        functools.partial(forward_kernel, taps),
        (inputs, before, ahead, mine, other, tap_rows, bias),
        [
            ((rows, 2 * width), f32),
            ((more + halo, width), bf16),
            block,
            stats,
            ((dp_count // 2, 2, features // dp_count, 2 * width), bf16),
            ((dp_count // 2, 2, features // dp_count, width), bf16),
        ],
        scratch,
    )
    w_in, w_last = w_in.reshape(features, 2 * width), w_last.reshape(features, width)
    d_activated = jnp.dot(d_out, w_last, preferred_element_type=f32)
    d_edge = jnp.dot(ahead[halo:], w_last, preferred_element_type=f32)
    total = exchanged(sums, "sp")
    normed, d_normed, activated, sums, small = local(
        functools.partial(norm_kernel, channels),
        (conved, total, gain, beta, d_activated, d_edge),
        [block, block, ((rows, width), bf16), stats, ((8, width), f32)],
    )
    back = exchanged(sums, "sp")
    piece = rows // sp_count
    up, down, rest, d_both, d_conved = local(
        functools.partial(backward_kernel, taps, channels),
        (normed, d_normed, total, back, tap_rows, pre, w_in),
        [
            ((2, piece, features), bf16),
            ((2, piece, features), bf16),
            (((sp_count - 4) * piece, 2 * width), bf16),
            ((rows, 2 * width), bf16),
            ((rows, width), f32),
        ],
        scratch + [pltpu.VMEM((sp_count, piece, 2 * width), bf16)],
    )
    parts, begun = summed_over_sp(up, down, rest, piece, w_in)
    grad_input = gathered_over_sp(parts)

    small, d_both = local(
        functools.partial(taps_kernel, taps),
        (d_conved, gated, small, d_both, begun),
        [((40, width), bf16), (d_both.shape, bf16)],
        scratch,
        in_specs=[VMEM] * 4 + [ANY],
    )
    per_device = features // dp_count
    (sent,) = local(
        pack_kernel,
        (row_terms(inputs, d_both).astype(bf16), row_terms(d_out, activated).astype(bf16), small),
        [((dp_count, 3 * per_device + small.shape[0], width), bf16)],
    )
    received = exchanged(sent, "dp")
    shapes = [((n, width), f32) for n in [per_device] * 3 + [taps] + [1] * 3]
    *grads, for_bias, for_gain, for_beta = local(final_kernel, (received,), shapes)
    return (grad_input, *grads, *(x.reshape(width) for x in (for_bias, for_gain, for_beta)))


def solution(mesh):
    rows, tile, lane = P("dp", None), P("dp", "sp"), P("sp")
    in_specs = (rows, tile, tile, P(None, "sp"), lane, lane, lane, tile, rows)
    out_specs = (rows, tile, tile, tile, P(None, "sp"), lane, lane, lane)
    return jax.shard_map(body, mesh=mesh, in_specs=in_specs, out_specs=out_specs, check_vma=False)
```

```python
import functools

import jax
import jax.numpy as jnp
from jax import lax
from jax.experimental import pallas as pl
from jax.experimental.pallas import tpu as pltpu
from jax.sharding import PartitionSpec as P


norm_eps = 1e-05
bf16 = jnp.bfloat16
f32 = jnp.float32
halo = 32
VMEM = pl.BlockSpec(memory_space=pltpu.VMEM)
ANY = pl.BlockSpec(memory_space=pl.ANY)


def shifted(block, axis, distance):
    count = lax.axis_size(axis)
    route = [(i - distance, i) for i in range(count) if 0 <= i - distance < count]
    return lax.ppermute(block, axis, route)


def side():
    return 1 - 2 * lax.rem(lax.axis_index("dp"), 2)


def turned(block, distance):
    sp_count, dp_count = lax.axis_size("sp"), lax.axis_size("dp")
    route = [
        (i * dp_count + j, (i + (1 - 2 * (j % 2)) * distance) % sp_count * dp_count + j)
        for i in range(sp_count)
        for j in range(dp_count)
    ]
    return lax.ppermute(block, ("sp", "dp"), route)


def exchanged(copies, axis):
    return lax.all_to_all(copies, axis, split_axis=0, concat_axis=0, tiled=True)


def row_terms(left_full, right_block):
    return lax.dot_general(
        left_full, right_block, (((0,), (0,)), ((), ())), preferred_element_type=f32
    )


def plus(*terms):
    total = terms[0].astype(f32)
    for term in terms[1:]:
        total = total + term.astype(f32)
    return total.astype(bf16)


def logistic(x):
    return 1.0 / (1.0 + jnp.exp(-x))


def put_lane_sums(out_ref, first, second):
    ones = jnp.ones((8, first.shape[1]), f32)
    dims = (((1,), (1,)), ((), ()))
    rows = first.shape[0]
    out_ref[...] = jnp.zeros(out_ref.shape, f32)
    for at, x in ((0, first), (out_ref.shape[2] // 2, second)):
        sums = lax.dot_general(
            ones, x, dims, preferred_element_type=f32, precision=lax.Precision.HIGHEST
        )[0:1]
        for k in range(out_ref.shape[0]):
            out_ref[k, :, at : at + rows] = sums


def both_totals(parts_ref):
    total = jnp.sum(parts_ref[...], axis=0)
    rows = total.shape[1] // 2
    return total[:, :rows], total[:, rows:]


def columns(first, second, rows):
    shape = (8, first.shape[1])
    row = lax.broadcasted_iota(jnp.int32, shape, 0)
    both = jnp.where(row == 0, jnp.broadcast_to(first, shape), jnp.broadcast_to(second, shape)).T
    return both[:rows, 0:1], both[:rows, 1:2]


def all_shifts(ext_ref, sh_ref):
    length = ext_ref.shape[0] - 8
    for r in range(8):
        sh_ref[r, 0:length, :] = ext_ref[r : r + length, :]


def window(sh_ref, offset, start, size):
    base = offset // 8 * 8 + start
    return sh_ref[offset % 8, base : base + size, :]


def convolve(sh_ref, taps_ref, offsets, rows, piece, put):
    for start in range(0, rows, piece):
        total = None
        for k, offset in offsets:
            term = window(sh_ref, offset, start, piece) * taps_ref[k : k + 1, :]
            total = term if total is None else total + term
        put(start, total)


def forward_kernel(taps, x_ref, before_ref, ahead_ref, mine_ref, other_ref, taps_ref, bias_ref, pre_ref, gated_ref, conved_ref, stats_ref, first_ref, last_ref, ext_ref, sh_ref):
    length, width = gated_ref.shape
    _, features = x_ref.shape
    core = lax.rem(lax.axis_index("dp"), 2)
    for k in range(first_ref.shape[0]):
        for ref, at in ((mine_ref, core), (other_ref, 1 - core)):
            first_ref[k, at] = ref[k, :, : 2 * width]
            last_ref[k, at] = ref[k, :, 2 * width :]
    weights = first_ref[...].reshape(features, 2 * width)
    edges = jnp.concatenate([before_ref[...], ahead_ref[0:halo]])
    edges = jnp.dot(edges, weights, preferred_element_type=f32)
    own = jnp.dot(x_ref[...], weights, preferred_element_type=f32)
    pre_ref[...] = own
    pre = jnp.concatenate([edges[:halo], own, edges[halo:]])
    gated = (pre[:, :width] * logistic(pre[:, width:])).astype(bf16)
    gated_ref[...] = gated
    ext_ref[0:length, :] = gated.astype(f32)
    ext_ref[length:, :] = jnp.zeros((8, width), f32)
    all_shifts(ext_ref, sh_ref)

    def put(start, total):
        conved_ref[start : start + 104, :] = total + bias_ref[...]

    more = conved_ref.shape[0]
    convolve(sh_ref, taps_ref, [(k, halo - taps + 1 + k) for k in range(taps)], more, 104, put)
    conved = conved_ref[...]
    put_lane_sums(stats_ref, conved, conved * conved)


def scales(total_ref, channels, rows):
    first, second = both_totals(total_ref)
    row_mean = first / channels
    row_spread = second / channels - row_mean * row_mean
    return columns(row_mean, lax.rsqrt(row_spread + norm_eps), rows)


def norm_kernel(channels, conved_ref, total_ref, gain_ref, beta_ref, d_act_ref, d_edge_ref, normed_ref, d_normed_ref, act_ref, stats_ref, small_ref):
    own = act_ref.shape[0]
    row_mean, inv_scale = scales(total_ref, channels, conved_ref.shape[0])
    normed = (conved_ref[...] - row_mean) * inv_scale
    gain = gain_ref[...]
    pre_act = normed * gain + beta_ref[...]
    sig = logistic(pre_act)
    act_ref[...] = (pre_act[:own] * sig[:own]).astype(bf16)
    d_act = jnp.concatenate([d_act_ref[...], d_edge_ref[...]])
    d_shifted = d_act * (sig * (1.0 + pre_act * (1.0 - sig)))
    d_normed = d_shifted * gain
    normed_ref[...] = normed
    d_normed_ref[...] = d_normed
    put_lane_sums(stats_ref, d_normed, d_normed * normed)
    shape = small_ref.shape
    row = lax.broadcasted_iota(jnp.int32, shape, 0)
    by_gain = jnp.sum(d_shifted[:own] * normed[:own], axis=0, keepdims=True)
    by_beta = jnp.sum(d_shifted[:own], axis=0, keepdims=True)
    by_gain, by_beta = jnp.broadcast_to(by_gain, shape), jnp.broadcast_to(by_beta, shape)
    small_ref[...] = jnp.where(row == 0, by_gain, jnp.where(row == 1, by_beta, 0.0))


def place_of(b, a):
    late = jnp.where(b == 0, 4 + a, 8 + a)
    split = jnp.where(a < 2, a, 12 + a)
    return jnp.where(b == 3, split, jnp.where(b == 1, jnp.where(a < 2, 12 + a, a), late))


def backward_kernel(taps, channels, normed_ref, d_normed_ref, total_ref, back_ref, taps_ref, pre_ref, w_in_ref, up_ref, down_ref, rest_ref, natural_ref, d_conved_ref, ext_ref, sh_ref, out_ref):
    rows, width = d_conved_ref.shape
    blocks = out_ref.shape[0]
    _, inv_scale = scales(total_ref, channels, rows + halo)
    first, second = both_totals(back_ref)
    first, second = columns(first / channels, second / channels, rows + halo)
    d_conved = inv_scale * (d_normed_ref[...] - first - normed_ref[...] * second)
    d_conved_ref[...] = d_conved[:rows]
    ext_ref[0 : rows + halo, :] = d_conved
    ext_ref[rows + halo : rows + halo + 8, :] = jnp.zeros((8, width), f32)
    all_shifts(ext_ref, sh_ref)
    me, way = lax.axis_index("sp"), side()
    piece = rows // blocks

    def put(start, d_gated):
        at = slice(start, start + piece)
        value = pre_ref[at, :width]
        sig = logistic(pre_ref[at, width:])
        d_value = d_gated * sig
        d_gate = d_value * value * (1.0 - sig)
        both = jnp.concatenate([d_value, d_gate], axis=1).astype(bf16)
        away = lax.rem(way * (start // piece - me) + blocks, blocks)
        out_ref[place_of(lax.rem(away, 4), away // 4)] = both
        natural_ref[start : start + piece, :] = both

    convolve(sh_ref, taps_ref, [(k, taps - 1 - k) for k in range(taps)], rows, piece, put)
    head = jnp.concatenate([out_ref[k] for k in range(4)])
    head = lax.dot_general(
        head, w_in_ref[...], (((1,), (1,)), ((), ())), preferred_element_type=f32
    ).astype(bf16)
    for k in range(4):
        (up_ref if k < 2 else down_ref)[k % 2] = head[k * piece : (k + 1) * piece]
    for k in range(4, blocks):
        rest_ref[(k - 4) * piece : (k - 3) * piece, :] = out_ref[k]


def taps_kernel(taps, d_conved_ref, gated_ref, small_ref, out_ref, ext_ref, sh_ref):
    rows, width = d_conved_ref.shape
    ext_ref[0 : halo + rows, :] = gated_ref[0 : halo + rows, :].astype(f32)
    ext_ref[halo + rows : halo + rows + 8, :] = jnp.zeros((8, width), f32)
    all_shifts(ext_ref, sh_ref)

    def folded(x):
        return jnp.sum(x.reshape(rows // 8, 8, width), axis=0)

    d_conved = d_conved_ref[...]
    sums = [
        folded(d_conved * window(sh_ref, halo - taps + 1 + k, 0, rows)) for k in range(taps)
    ]
    sums.append(folded(d_conved))
    sums = [jnp.sum(s, axis=0, keepdims=True) for s in sums]
    out_ref[...] = jnp.concatenate(sums + [small_ref[...]], axis=0).astype(bf16)


def power_of_two(exponent):
    size = jnp.abs(exponent).astype(jnp.int32)
    up = down = jnp.ones(exponent.shape, f32)
    for bit in range(7):
        has = jnp.bitwise_and(size, 1 << bit) != 0
        up = up * jnp.where(has, f32(2.0 ** 2**bit), f32(1.0))
        down = down * jnp.where(has, f32(2.0 ** -(2**bit)), f32(1.0))
    return jnp.where(exponent < 0, down, up)


def total_kernel(*refs):
    *parts, out_ref = refs
    features = parts[0].shape[1]
    total = parts[0][...].astype(f32)
    for part in parts[1:]:
        total = total + part[...].astype(f32)
    total = total.astype(bf16).astype(f32)
    top = jnp.max(jnp.max(jnp.abs(total), axis=0, keepdims=True), axis=1, keepdims=True)
    top = jnp.broadcast_to(top, (8, 128))
    exponent = jnp.floor(jnp.log(jnp.maximum(top, 1e-37)) * 1.4426950408889634)
    exponent = 13.0 - jnp.clip(exponent, -113.0, 127.0)
    out_ref[:, :features] = (total * power_of_two(exponent)[0:1, 0:1]).astype(bf16)
    out_ref[:, features:] = jnp.broadcast_to(exponent[0:1], (out_ref.shape[0], 128)).astype(bf16)


def copies_kernel(*refs):
    *shards, out_ref, whole_ref, sem = refs
    at = 0
    for shard in shards:
        whole_ref[:, at : at + shard.shape[1]] = shard[...]
        at += shard.shape[1]
    copies = [
        pltpu.make_async_copy(whole_ref, out_ref.at[k], sem.at[k]) for k in range(out_ref.shape[0])
    ]
    for copy in copies:
        copy.start()
    for copy in copies:
        copy.wait()


def from_same_core(shards):
    count = lax.axis_size("dp")
    copies = copies_for_all(shards, count // 2)
    groups = [list(range(core, count, 2)) for core in range(2)]
    return lax.all_to_all(copies, "dp", 0, 0, tiled=True, axis_index_groups=groups)


def copies_for_all(shards, count):
    shape = (shards[0].shape[0], sum(s.shape[1] for s in shards))
    return pl.pallas_call(
        copies_kernel,
        out_shape=jax.ShapeDtypeStruct((count, *shape), shards[0].dtype),
        in_specs=[VMEM] * len(shards),
        out_specs=ANY,
        scratch_shapes=[pltpu.VMEM(shape, shards[0].dtype), pltpu.SemaphoreType.DMA((count,))],
    )(*shards)


def pack_kernel(both_ref, last_ref, small_ref, out_ref):
    slots, _, width = out_ref.shape
    each = both_ref.shape[0] // slots
    for k in range(slots):
        at = slice(k * each, (k + 1) * each)
        out_ref[k, 0:each] = both_ref[at, :width]
        out_ref[k, each : 2 * each] = both_ref[at, width:]
        out_ref[k, 2 * each : 3 * each] = last_ref[at]
        out_ref[k, 3 * each :] = small_ref[...]


def local(kernel, inputs, shapes, scratch=()):
    return pl.pallas_call(
        kernel,
        out_shape=[jax.ShapeDtypeStruct(s, t) for s, t in shapes],
        in_specs=[VMEM] * len(inputs),
        out_specs=[VMEM] * len(shapes),
        scratch_shapes=list(scratch),
        compiler_params=pltpu.CompilerParams(vmem_limit_bytes=20 * 2**20),
    )(*inputs)


def summed_over_sp(up, down, rest, rows, weights):
    def part(left):
        out = lax.dot_general(
            left,
            weights,
            (((1,), (1,)), ((), ())),
            preferred_element_type=f32,
        )
        return out.astype(bf16).reshape(-1, rows, out.shape[-1])

    up, down = turned(up, 1), turned(down, -1)
    rest = part(rest)
    far = turned(rest[2:3], 2)
    up = turned(jnp.stack([plus(rest[4], up[0]), plus(rest[5], up[1], far[0])]), 1)
    down = turned(plus(rest[6:8], down), -1)
    up = turned(plus(rest[8:10], up), 1)
    down = turned(plus(rest[10:12], down), -1)
    up_4 = turned(plus(rest[1], up[1]), 4)
    down_4 = turned(plus(rest[3], down[0]), -4)
    return (rest[0], up[0], down[1], up_4, down_4)


def gathered_over_sp(parts):
    rows, features = parts[0].shape
    (own,) = local(total_kernel, parts, [((rows, features + 128), bf16)])
    whole = lax.all_gather(own.astype(jnp.float16), "sp", axis=0, tiled=True)
    scale = power_of_two(-whole[:, features:].astype(f32))
    scale = lax.optimization_barrier(scale)
    return (whole[:, :features].astype(f32) * scale[:, :1]).astype(bf16)


def final_kernel(parts_ref, *out_refs):
    total = parts_ref[0].astype(f32)
    for k in range(1, parts_ref.shape[0]):
        total = total + parts_ref[k].astype(f32)
    at = 0
    for ref in out_refs:
        ref[...] = total[at : at + ref.shape[0]]
        at += ref.shape[0]


def body(inputs, w_value, w_gate, kernel, conv_bias, ln_gain, ln_bias, w_out, d_out):
    rows, features = inputs.shape
    width = w_value.shape[1]
    taps = kernel.shape[0]
    sp_count, dp_count = lax.axis_size("sp"), lax.axis_size("dp")
    channels = width * sp_count
    mine = from_same_core((w_value, w_gate, w_out))
    before = shifted(inputs[rows - halo :], "dp", 1)
    ahead = shifted(jnp.concatenate([inputs[:halo], d_out[:halo]]), "dp", -1)
    tap_rows = jnp.pad(kernel, ((0, 32 - taps), (0, 0))).astype(f32)
    lane = (1, width)
    bias, gain, beta = (x.astype(f32).reshape(lane) for x in (conv_bias, ln_gain, ln_bias))
    mine, before, ahead, tap_rows, bias, gain, beta = lax.optimization_barrier(
        (mine, before, ahead, tap_rows, bias, gain, beta)
    )
    other = lax.ppermute(mine, "dp", [(i, i ^ 1) for i in range(dp_count)])
    more = rows + halo
    stats_width = -(-more // 128) * 128
    block, stats = ((more, width), f32), ((sp_count, 1, 2 * stats_width), f32)
    scratch = [
        pltpu.VMEM((more + halo + 8, width), f32),
        pltpu.VMEM((8, more + halo, width), f32),
    ]
    pre, gated, conved, sums, w_in, w_last = local(
        functools.partial(forward_kernel, taps),
        (inputs, before, ahead, mine, other, tap_rows, bias),
        [
            ((rows, 2 * width), f32),
            ((more + halo, width), bf16),
            block,
            stats,
            ((dp_count // 2, 2, features // dp_count, 2 * width), bf16),
            ((dp_count // 2, 2, features // dp_count, width), bf16),
        ],
        scratch,
    )
    w_in, w_last = w_in.reshape(features, 2 * width), w_last.reshape(features, width)
    d_activated = jnp.dot(d_out, w_last, preferred_element_type=f32)
    d_edge = jnp.dot(ahead[halo:], w_last, preferred_element_type=f32)
    total = exchanged(sums, "sp")
    normed, d_normed, activated, sums, small = local(
        functools.partial(norm_kernel, channels),
        (conved, total, gain, beta, d_activated, d_edge),
        [block, block, ((rows, width), bf16), stats, ((8, width), f32)],
    )
    back = exchanged(sums, "sp")
    piece = rows // sp_count
    up, down, rest, d_both, d_conved = local(
        functools.partial(backward_kernel, taps, channels),
        (normed, d_normed, total, back, tap_rows, pre, w_in),
        [
            ((2, piece, features), bf16),
            ((2, piece, features), bf16),
            (((sp_count - 4) * piece, 2 * width), bf16),
            ((rows, 2 * width), bf16),
            ((rows, width), f32),
        ],
        scratch + [pltpu.VMEM((sp_count, piece, 2 * width), bf16)],
    )
    parts = summed_over_sp(up, down, rest, piece, w_in)
    grad_input = gathered_over_sp(parts)

    (small,) = local(
        functools.partial(taps_kernel, taps),
        (d_conved, gated, small),
        [((40, width), bf16)],
        scratch,
    )
    per_device = features // dp_count
    (sent,) = local(
        pack_kernel,
        (row_terms(inputs, d_both).astype(bf16), row_terms(d_out, activated).astype(bf16), small),
        [((dp_count, 3 * per_device + small.shape[0], width), bf16)],
    )
    received = exchanged(sent, "dp")
    shapes = [((n, width), f32) for n in [per_device] * 3 + [taps] + [1] * 3]
    *grads, for_bias, for_gain, for_beta = local(final_kernel, (received,), shapes)
    return (grad_input, *grads, *(x.reshape(width) for x in (for_bias, for_gain, for_beta)))


def solution(mesh):
    rows, tile, lane = P("dp", None), P("dp", "sp"), P("sp")
    in_specs = (rows, tile, tile, P(None, "sp"), lane, lane, lane, tile, rows)
    out_specs = (rows, tile, tile, tile, P(None, "sp"), lane, lane, lane)
    return jax.shard_map(body, mesh=mesh, in_specs=in_specs, out_specs=out_specs, check_vma=False)
```
